32 devices in a mesh: pp: 4 (over y, x), fs: 4 (over z), tp: 2 (over core).
Axes of the slice: x: 2, y: 2, z: 4, core: 2. Of those that a mesh axis runs over, the one named last changes fastest.
Arguments:
- micro_in: bfloat16 [2, 96, 1024], P(None, 'pp', ('tp', 'fs')), may hold values from -6 to 6
- norm_gain: float32 [4, 1024], P('pp'), may hold values from 0.5 to 1.5
- proj_gate: bfloat16 [4, 1024, 8, 4, 64], P('pp', None, 'tp', 'fs'), may hold values from -0.1875 to 0.1875
- proj_value: bfloat16 [4, 1024, 8, 4, 64], P('pp', None, 'tp', 'fs'), may hold values from -0.1875 to 0.1875
- proj_write: bfloat16 [4, 1024, 8, 128], P('pp', None, 'tp'), may hold values from -0.1875 to 0.1875
- proj_read: bfloat16 [4, 1024, 8, 128], P('pp', None, 'tp'), may hold values from -0.1875 to 0.1875
- proj_step: bfloat16 [4, 1024, 2, 8, 4], P('pp', None, None, 'tp', 'fs'), may hold values from -0.1875 to 0.1875
- step_bias: float32 [4, 2, 8, 4], P('pp', None, 'tp', 'fs'), may hold values from -4.6 to -2.3
- decay_log: float32 [4, 2, 8, 4], P('pp', None, 'tp', 'fs'), may hold values from 0 to 2.77
- skip_gain: float32 [4, 8, 4], P('pp', 'tp', 'fs'), may hold values from 0.5 to 1.5
- conv_value: float32 [4, 5, 8, 4, 64], P('pp', None, 'tp', 'fs'), may hold values from -2.5 to 2.5
- conv_write: float32 [4, 5, 8, 128], P('pp', None, 'tp'), may hold values from -2.5 to 2.5
- conv_read: float32 [4, 5, 8, 128], P('pp', None, 'tp'), may hold values from -2.5 to 2.5
- proj_out: bfloat16 [4, 8, 4, 64, 1024], P('pp', 'tp', 'fs'), may hold values from -0.125 to 0.125
Outputs:
- mixed_out: bfloat16 [2, 96, 1024], P(None, 'pp', ('tp', 'fs'))
The draws below stay inside these ranges and needn't reach their ends.
All inputs are finite; a program needn't handle non-finite values.
Results may differ from the reference program's by a relative error of at most 0.025.
Values may be sent and summed in bfloat16 or wider, within the bound.
A program may use at most 64 MiB of HBM per device.

```python
import jax
import jax.numpy as jnp
from jax import lax

D = 1024
GROUPS = 8
PER_GROUP = 4
HEAD = 64
STATE = 128
TAPS = 5
TOK = 96
SECTIONS = 4
MICRO = 2
INNER = 2048


def block_scale(key, shape, pieces, low, top_value):
    factor_of, own = 1.0, jax.random.fold_in(key, 6)
    for dim, shards_of in pieces:
        steps = jnp.exp(jax.random.uniform(jax.random.fold_in(own, dim), (shards_of,), jnp.float32, low / len(pieces), top_value / len(pieces)))
        factor_of = factor_of * jnp.repeat(steps, shape[dim] // shards_of).reshape([-1 if axis == dim else 1 for axis in range(len(shape))])
    return factor_of


def gaussian(stream_key, extent, scale, limit, split=(), held_as=jnp.bfloat16):
    factor_of = block_scale(stream_key, extent, split, -0.22, 0.18) if split else 1.0
    entries = jax.random.normal(stream_key, extent, jnp.float32) * scale * factor_of
    return jnp.minimum(jnp.maximum(entries, -limit), limit).astype(held_as)


def setup_inputs(seed: int = 0) -> dict:
    key_of = jax.random.split(jax.random.key(seed), 15)
    return {
        "micro_in": gaussian(key_of[0], (MICRO, TOK, D), 1.0, 6.0, ((1, 4), (2, 8))),
        "norm_gain": jnp.clip(1.0 + 0.1 * jax.random.normal(key_of[1], (SECTIONS, D), jnp.float32), 0.5, 1.5),
        "proj_gate": gaussian(key_of[2], (SECTIONS, D, GROUPS, PER_GROUP, HEAD), D ** -0.5, 0.1875, ((0, 4), (2, 2), (3, 4))),
        "proj_value": gaussian(key_of[3], (SECTIONS, D, GROUPS, PER_GROUP, HEAD), D ** -0.5, 0.1875, ((0, 4), (2, 2), (3, 4))),
        "proj_write": gaussian(key_of[4], (SECTIONS, D, GROUPS, STATE), D ** -0.5, 0.1875, ((0, 4), (2, 2))),
        "proj_read": gaussian(key_of[5], (SECTIONS, D, GROUPS, STATE), D ** -0.5, 0.1875, ((0, 4), (2, 2))),
        "proj_step": gaussian(key_of[6], (SECTIONS, D, 2, GROUPS, PER_GROUP), D ** -0.5, 0.1875, ((0, 4), (3, 2), (4, 4))),
        "step_bias": jnp.clip(-4.6 + 2.3 * jax.random.uniform(key_of[7], (SECTIONS, 2, GROUPS, PER_GROUP), jnp.float32) ** block_scale(key_of[7], (SECTIONS, 2, GROUPS, PER_GROUP), ((0, 4), (2, 2), (3, 4)), -0.2, 0.2), -4.6, -2.3),
        "decay_log": jnp.clip(2.77 * jax.random.uniform(key_of[8], (SECTIONS, 2, GROUPS, PER_GROUP), jnp.float32) ** block_scale(key_of[8], (SECTIONS, 2, GROUPS, PER_GROUP), ((0, 4), (2, 2), (3, 4)), -0.2, 0.2), 0.0, 2.77),
        "skip_gain": jnp.clip(1.0 + 0.1 * jax.random.normal(key_of[9], (SECTIONS, GROUPS, PER_GROUP), jnp.float32), 0.5, 1.5),
        "conv_value": gaussian(key_of[10], (SECTIONS, TAPS, GROUPS, PER_GROUP, HEAD), TAPS ** -0.5, 2.5, ((0, 4), (2, 2), (3, 4)), jnp.float32),
        "conv_write": gaussian(key_of[11], (SECTIONS, TAPS, GROUPS, STATE), TAPS ** -0.5, 2.5, ((0, 4), (2, 2)), jnp.float32),
        "conv_read": gaussian(key_of[12], (SECTIONS, TAPS, GROUPS, STATE), TAPS ** -0.5, 2.5, ((0, 4), (2, 2)), jnp.float32),
        "proj_out": gaussian(key_of[13], (SECTIONS, GROUPS, PER_GROUP, HEAD, D), INNER ** -0.5, 0.125, ((0, 4), (1, 2), (2, 4))),
    }


epsilon = 1e-06

def centred_conv(signal, conv_taps):
    span_width = conv_taps.shape[0]
    half_width = span_width // 2
    length = signal.shape[0]
    padded = jnp.pad(signal, ((half_width, half_width), (0, 0)))
    running = jnp.zeros_like(signal)
    for offset in range(span_width):
        running = running + padded[offset:offset + length] * conv_taps[offset]
    return running

def duality_mix(gate_flat, value_flat, write_flat, read_flat, step_raw, step_bias, decay_log, skip_gain, conv_value, conv_write, conv_read):
    groups, per_group = skip_gain.shape
    length = gate_flat.shape[0]
    head_size = value_flat.shape[1] // (groups * per_group)
    state_size = write_flat.shape[1] // groups
    taps_count = conv_value.shape[0]
    value_act = jax.nn.silu(centred_conv(value_flat.astype(jnp.float32), conv_value.reshape(taps_count, -1))).astype(jnp.bfloat16)
    write_act = jax.nn.silu(centred_conv(write_flat.astype(jnp.float32), conv_write.reshape(taps_count, -1))).astype(jnp.bfloat16)
    read_act = jax.nn.silu(centred_conv(read_flat.astype(jnp.float32), conv_read.reshape(taps_count, -1))).astype(jnp.bfloat16)
    step_size = jax.nn.softplus(step_raw.reshape(length, 2, groups, per_group) + step_bias[None])
    log_decay = step_size * (-jnp.exp(decay_log))[None]
    fwd_cum = jnp.cumsum(log_decay[:, 0], axis=0)
    bwd_cum = jnp.flip(jnp.cumsum(jnp.flip(log_decay[:, 1], 0), axis=0), 0)
    positions = jnp.arange(length)
    lower_mask = (positions[:, None] >= positions[None, :])[:, :, None, None]
    upper_mask = (positions[:, None] <= positions[None, :])[:, :, None, None]
    fwd_weight = jnp.exp(jnp.where(lower_mask, fwd_cum[:, None] - fwd_cum[None, :], -jnp.inf)) * step_size[None, :, 0]
    bwd_weight = jnp.exp(jnp.where(upper_mask, bwd_cum[:, None] - bwd_cum[None, :], -jnp.inf)) * step_size[None, :, 1]
    scores = jnp.einsum('tgn,sgn->tsg', read_act.reshape(length, groups, state_size).astype(jnp.float32), write_act.reshape(length, groups, state_size).astype(jnp.float32), precision=lax.Precision.HIGHEST)
    combined = scores[:, :, :, None] * (fwd_weight + bwd_weight)
    value_heads = value_act.reshape(length, groups, per_group, head_size).astype(jnp.float32)
    mixed_heads = jnp.einsum('tsgh,sghp->tghp', combined, value_heads, precision=lax.Precision.HIGHEST)
    mixed_heads = mixed_heads + skip_gain[None, :, :, None] * value_heads
    return (mixed_heads.reshape(length, -1) * jax.nn.silu(gate_flat.astype(jnp.float32))).astype(jnp.bfloat16)

def section_apply(tokens, norm_gain, proj_gate, proj_value, proj_write, proj_read, proj_step, step_bias, decay_log, skip_gain, conv_value, conv_write, conv_read, proj_out):
    width_model = tokens.shape[1]
    as_float = tokens.astype(jnp.float32)
    scale_rms = lax.rsqrt(lax.optimization_barrier(jnp.mean(as_float * as_float, axis=1, keepdims=True)) + epsilon)
    normed = (as_float * scale_rms * norm_gain[None, :]).astype(jnp.bfloat16)
    gate_flat = jnp.dot(normed, proj_gate.reshape(width_model, -1), preferred_element_type=jnp.float32).astype(jnp.bfloat16)
    value_flat = jnp.dot(normed, proj_value.reshape(width_model, -1), preferred_element_type=jnp.float32).astype(jnp.bfloat16)
    write_flat = jnp.dot(normed, proj_write.reshape(width_model, -1), preferred_element_type=jnp.float32).astype(jnp.bfloat16)
    read_flat = jnp.dot(normed, proj_read.reshape(width_model, -1), preferred_element_type=jnp.float32).astype(jnp.bfloat16)
    step_raw = jnp.dot(normed, proj_step.reshape(width_model, -1), preferred_element_type=jnp.float32)
    gated_out = duality_mix(gate_flat, value_flat, write_flat, read_flat, step_raw, step_bias, decay_log, skip_gain, conv_value, conv_write, conv_read)
    branch = jnp.dot(gated_out, proj_out.reshape(-1, width_model), preferred_element_type=jnp.float32).astype(jnp.bfloat16)
    branch = lax.optimization_barrier(branch)
    return (as_float + 0.5 * branch.astype(jnp.float32)).astype(jnp.bfloat16)

def reference(micro_in, norm_gain, proj_gate, proj_value, proj_write, proj_read, proj_step, step_bias, decay_log, skip_gain, conv_value, conv_write, conv_read, proj_out):
    weights = (norm_gain, proj_gate, proj_value, proj_write, proj_read, proj_step, step_bias, decay_log, skip_gain, conv_value, conv_write, conv_read, proj_out)

    def run_section(current, section_weights):
        return (section_apply(current, *section_weights), None)

    def one_micro(tokens):
        final_section, unused = lax.scan(run_section, tokens, weights)
        as_float = final_section.astype(jnp.float32)
        scale_rms = lax.rsqrt(lax.optimization_barrier(jnp.mean(as_float * as_float, axis=1, keepdims=True)) + epsilon)
        return (as_float * scale_rms).astype(jnp.bfloat16)
    return lax.map(one_micro, micro_in)
```

```python
import functools

import jax
import jax.numpy as jnp
from jax import lax
from jax.experimental import pallas as pl
from jax.experimental.pallas import tpu as pltpu
from jax.sharding import PartitionSpec as P

epsilon = 1e-06


def own_rows_2(portion, span, axis):
    count = span * lax.axis_size(axis)
    sent = portion(jnp.int32(0), count).astype(jnp.bfloat16)
    return lax.psum_scatter(sent, axis, scatter_dimension=0, tiled=True).astype(jnp.float32)


def from_behind(block, axis, distance):
    devices = range(lax.axis_size(axis))
    route = [(i - distance, i) for i in devices if i - distance in devices]
    return lax.ppermute(block, axis, route)


def spread(value, axis, source):
    kept = jnp.where(lax.axis_index(axis) == source, value, 0).astype(value.dtype)
    return lax.psum(kept, axis)


def centred_conv(signal, conv_taps):
    span_width = conv_taps.shape[0]
    half_width = span_width // 2
    length = signal.shape[0]
    padded = jnp.pad(signal, ((half_width, half_width), (0, 0)))
    running = jnp.zeros_like(signal)
    for offset in range(span_width):
        running = running + padded[offset : offset + length] * conv_taps[offset]
    return running


def duality_mix(
    gate_flat,
    value_flat,
    write_flat,
    read_flat,
    step_raw,
    step_bias,
    decay_log,
    skip_gain,
    conv_value,
    conv_write,
    conv_read,
):
    groups, per_group = skip_gain.shape
    length = gate_flat.shape[0]
    head_size = value_flat.shape[1] // (groups * per_group)
    state_size = write_flat.shape[1] // groups
    taps_count = conv_value.shape[0]
    value_act = jax.nn.silu(
        centred_conv(value_flat.astype(jnp.float32), conv_value.reshape(taps_count, -1))
    ).astype(jnp.bfloat16)
    write_act = jax.nn.silu(
        centred_conv(write_flat.astype(jnp.float32), conv_write.reshape(taps_count, -1))
    ).astype(jnp.bfloat16)
    read_act = jax.nn.silu(
        centred_conv(read_flat.astype(jnp.float32), conv_read.reshape(taps_count, -1))
    ).astype(jnp.bfloat16)
    step_size = jax.nn.softplus(step_raw.reshape(length, 2, groups, per_group) + step_bias[None])
    log_decay = step_size * (-jnp.exp(decay_log))[None]
    fwd_cum = jnp.cumsum(log_decay[:, 0], axis=0)
    bwd_cum = jnp.flip(jnp.cumsum(jnp.flip(log_decay[:, 1], 0), axis=0), 0)
    positions = jnp.arange(length)
    lower_mask = (positions[:, None] >= positions[None, :])[:, :, None, None]
    upper_mask = (positions[:, None] <= positions[None, :])[:, :, None, None]
    fwd_weight = (
        jnp.exp(jnp.where(lower_mask, fwd_cum[:, None] - fwd_cum[None, :], -jnp.inf))
        * step_size[None, :, 0]
    )
    bwd_weight = (
        jnp.exp(jnp.where(upper_mask, bwd_cum[:, None] - bwd_cum[None, :], -jnp.inf))
        * step_size[None, :, 1]
    )
    scores = jnp.einsum(
        "tgn,sgn->tsg",
        read_act.reshape(length, groups, state_size),
        write_act.reshape(length, groups, state_size),
        preferred_element_type=jnp.float32,
    )
    combined = scores[:, :, :, None] * (fwd_weight + bwd_weight)
    value_heads = value_act.reshape(length, groups, per_group, head_size).astype(jnp.float32)
    mixed_heads = jnp.einsum(
        "tsgh,sghp->tghp", combined, value_heads, precision=lax.Precision.HIGHEST
    )
    mixed_heads = mixed_heads + skip_gain[None, :, :, None] * value_heads
    return (mixed_heads.reshape(length, -1) * jax.nn.silu(gate_flat.astype(jnp.float32))).astype(
        jnp.bfloat16
    )


def body(
    micro_in,
    norm_gain,
    proj_gate,
    proj_value,
    proj_write,
    proj_read,
    proj_step,
    step_bias,
    decay_log,
    skip_gain,
    conv_value,
    conv_write,
    conv_read,
    proj_out,
):
    section_count = lax.axis_size("pp")
    section_idx = lax.axis_index("pp")
    width_model = norm_gain.shape[1]
    fed_blocks = lax.all_gather(micro_in, "pp", axis=1, tiled=True)
    micro_count = fed_blocks.shape[0]
    length = fed_blocks.shape[1]
    fed_columns = jnp.swapaxes(fed_blocks, 1, 2)
    gain_vec = norm_gain[0].astype(jnp.float32)
    cut_gate = proj_gate.shape[2] * proj_gate.shape[3] * proj_gate.shape[4]
    cut_write = proj_write.shape[2] * proj_write.shape[3]
    weight_all = jnp.concatenate(
        [
            proj_gate[0].reshape(width_model, -1),
            proj_value[0].reshape(width_model, -1),
            proj_write[0].reshape(width_model, -1),
            proj_read[0].reshape(width_model, -1),
            proj_step[0].reshape(width_model, -1),
        ],
        axis=1,
    )
    out_weights = proj_out[0].reshape(-1, width_model)
    own_rows = width_model // lax.axis_size(("tp", "fs"))

    def project(column_block):
        gathered = lax.all_gather(column_block, ("tp", "fs"), axis=0, tiled=True)
        as_float = gathered.astype(jnp.float32)
        scale_rms = lax.rsqrt(jnp.mean(as_float * as_float, axis=0) + epsilon)
        normed = (as_float * scale_rms[None, :] * gain_vec[:, None]).astype(jnp.bfloat16)
        return lax.dot_general(
            normed, weight_all, (((0,), (0,)), ((), ())), preferred_element_type=jnp.float32
        )

    def term_maker(token_rows):

        def term_rows(offset, span_count):
            weight_cols = lax.dynamic_slice_in_dim(out_weights, offset, span_count, 1)
            return lax.dot_general(
                weight_cols,
                token_rows,
                (((0,), (1,)), ((), ())),
                preferred_element_type=jnp.float32,
            )

        return term_rows

    def mix_block(column_block):
        projected = project(column_block)
        gate_flat = projected[:, :cut_gate].astype(jnp.bfloat16)
        value_flat = projected[:, cut_gate : 2 * cut_gate].astype(jnp.bfloat16)
        write_flat = projected[:, 2 * cut_gate : 2 * cut_gate + cut_write].astype(jnp.bfloat16)
        read_flat = projected[:, 2 * cut_gate + cut_write : 2 * cut_gate + 2 * cut_write].astype(
            jnp.bfloat16
        )
        step_raw = projected[:, 2 * cut_gate + 2 * cut_write :]
        gated_out = duality_mix(
            gate_flat,
            value_flat,
            write_flat,
            read_flat,
            step_raw,
            step_bias[0],
            decay_log[0],
            skip_gain[0],
            conv_value[0],
            conv_write[0],
            conv_read[0],
        )
        summed = own_rows_2(term_maker(gated_out), own_rows, ("tp", "fs"))
        branch = lax.optimization_barrier(summed.astype(jnp.bfloat16))
        return (column_block.astype(jnp.float32) + 0.5 * branch.astype(jnp.float32)).astype(
            jnp.bfloat16
        )

    total_steps = micro_count + section_count - 1

    def advance(moment, loop_state):
        arriving, collected = loop_state
        pick_index = jnp.clip(moment, 0, micro_count - 1)
        fresh_block = lax.dynamic_index_in_dim(fed_columns, pick_index, 0, keepdims=False)
        current = jnp.where(section_idx == 0, fresh_block, arriving)
        produced = mix_block(current)
        slot_index = moment - section_idx
        keep_flag = (
            (section_idx == section_count - 1) & (slot_index >= 0) & (slot_index < micro_count)
        )
        slot_safe = jnp.clip(slot_index, 0, micro_count - 1)
        previous = lax.dynamic_index_in_dim(collected, slot_safe, 0, keepdims=False)
        collected = lax.dynamic_update_index_in_dim(
            collected, jnp.where(keep_flag, produced, previous), slot_safe, 0
        )
        arriving = from_behind(produced, "pp", 1)
        return (arriving, collected)

    start_loop = (jnp.zeros_like(fed_columns[0]), jnp.zeros_like(fed_columns))
    arriving, collected = lax.fori_loop(0, total_steps, advance, start_loop)
    shared = spread(collected, "pp", section_count - 1)
    token_share = length // section_count
    own_block = lax.dynamic_slice_in_dim(shared, section_idx * token_share, token_share, 2)
    as_float = own_block.astype(jnp.float32)
    partial_squares = jnp.sum(as_float * as_float, axis=1)
    total_squares = lax.psum(partial_squares, ("tp", "fs"))
    scale_rms = lax.rsqrt(total_squares / width_model + epsilon)
    result = (as_float * scale_rms[:, None, :]).astype(jnp.bfloat16)
    return jnp.swapaxes(result, 1, 2)


MESH = pl.DeviceIdType.MESH
NT_DIMS = (((1,), (1,)), ((), ()))
NN_DIMS = (((1,), (0,)), ((), ()))


def silu(x):
    return 0.5 * x * (1.0 + jnp.tanh(0.5 * x))


def matmul(left, right, dims=NN_DIMS, precision=None):
    return lax.dot_general(
        left, right, dims, precision=precision, preferred_element_type=jnp.float32
    )


def relay_kernel(
    sizes,
    in_ref,
    gain_ref,
    gate_w,
    value_w,
    write_w,
    read_w,
    step_w,
    bias_ref,
    decay_ref,
    skip_ref,
    tap_v,
    tap_w,
    tap_r,
    out_w,
    out_ref,
    entry,
    acts,
    partial,
    arrived,
    produced,
    leaving,
    final_in,
    squares,
    square_in,
    column,
    padded,
    sem_entry_s,
    sem_entry_r,
    sem_rs_s,
    sem_rs_r,
    sem_hop_s,
    sem_ag_r,
    sem_twin_s,
    sem_fin_s,
    sem_fin_r,
    sem_sq_s,
    sem_sq_r,
    sem_local,
):
    sections, ring, cores = sizes["pp"], sizes["fs"], sizes["tp"]
    owners = ring * cores
    micro, share, block = in_ref.shape
    length = share * sections
    width = owners * block
    inner = gate_w.shape[0]
    groups, state = tap_w.shape[1], tap_w.shape[2]
    taps, heads, head = tap_v.shape
    per_group = heads // groups
    half = taps // 2
    s = lax.axis_index("pp")
    z = lax.axis_index("fs")
    c = lax.axis_index("tp")
    j = c * ring + z
    last = sections - 1
    me = s * owners + j

    def place(section, owner):
        return {"pp": section, "fs": lax.rem(owner, ring), "tp": owner // ring}

    barrier = pltpu.get_barrier_semaphore()
    for step in range(1, sections * owners):
        other = lax.rem(me + step, sections * owners)
        pl.semaphore_signal(
            barrier,
            inc=1,
            device_id=place(other // owners, lax.rem(other, owners)),
            device_id_type=MESH,
        )
    pl.semaphore_wait(barrier, sections * owners - 1)

    def remote(src, dst, send_sem, recv_sem, target):
        return pltpu.make_async_remote_copy(
            src_ref=src,
            dst_ref=dst,
            send_sem=send_sem,
            recv_sem=recv_sem,
            device_id=target,
            device_id_type=MESH,
        )

    def entry_copy(m, step):
        owner = lax.rem(j + step, owners)
        return remote(
            in_ref.at[m],
            entry.at[m, j, s],
            sem_entry_s.at[m, step],
            sem_entry_r.at[m, j, s],
            place(0, owner),
        )

    def entry_own(m):
        return pltpu.make_async_copy(in_ref.at[m], entry.at[m, j, s], sem_entry_r.at[m, j, s])

    for m in range(micro):
        for step in range(1, owners):
            entry_copy(m, step).start()

        @pl.when(s == 0)
        def _():
            entry_own(m).start()

        @pl.when(s != 0)
        def _():
            entry_copy(m, 0).start()

    lane_v = lax.broadcasted_iota(jnp.int32, (1, heads * head), 1)
    row8 = lax.broadcasted_iota(jnp.int32, (2 * heads, 1), 0)
    bias_col = jnp.zeros((2 * heads, 1), jnp.float32)
    decay_col = jnp.zeros((2 * heads, 1), jnp.float32)
    skip_row = jnp.zeros((1, heads * head), jnp.float32)
    for i in range(2 * heads):
        d, h = i // heads, i % heads
        bias_col = jnp.where(row8 == i, bias_ref[d, h], bias_col)
        decay_col = jnp.where(row8 == i, decay_ref[d, h], decay_col)
    for h in range(heads):
        skip_row = jnp.where(lane_v // head == h, skip_ref[h], skip_row)
    decay_col = -jnp.exp(decay_col)
    value_taps = [
        jnp.concatenate([tap_v[k, h : h + 1, :] for h in range(heads)], axis=1)
        for k in range(taps)
    ]
    tpos = lax.broadcasted_iota(jnp.int32, (length, length), 0)
    spos = lax.broadcasted_iota(jnp.int32, (length, length), 1)
    lower = spos <= tpos
    diag = spos == tpos
    tri_low = jnp.where(lower, 1.0, 0.0)
    tri_up = jnp.where(spos >= tpos, 1.0, 0.0)
    edge = jnp.zeros((8, 128), jnp.float32)
    for q in range(padded.shape[0]):
        padded[q, 0:8, :] = edge
        padded[q, 8 + length : 16 + length, :] = edge

    def conv_act(slot, signal, rows):
        padded[slot, 8 : 8 + length, :] = signal.astype(jnp.bfloat16).astype(jnp.float32)
        start = 8 - half
        total = padded[slot, start : start + length, :] * rows[0]
        for k in range(1, taps):
            total = total + padded[slot, start + k : start + k + length, :] * rows[k]
        return silu(total).astype(jnp.bfloat16)

    def twin_copy(m, zz, step):
        slot = c * ring + zz
        other = lax.rem(c + step, cores)
        return remote(
            acts.at[m, slot],
            acts.at[m, slot],
            sem_twin_s.at[m, zz, step - 1],
            sem_ag_r.at[m, slot],
            {"pp": s, "fs": z, "tp": other},
        )

    def wait_block(m, slot):
        remote(
            acts.at[m, slot],
            acts.at[m, slot],
            sem_twin_s.at[m, 0, 0],
            sem_ag_r.at[m, slot],
            place(s, slot),
        ).wait_recv()

    def receive(m):
        @pl.when(s == 0)
        def _():
            for k in range(owners):
                for p in range(sections):
                    pltpu.make_async_copy(
                        in_ref.at[m], entry.at[m, k, p], sem_entry_r.at[m, k, p]
                    ).wait()
            for k in range(owners):
                acts[m, k] = jnp.concatenate(
                    [entry[m, k, p].astype(jnp.float32) for p in range(sections)], axis=0
                ).astype(jnp.bfloat16)

        @pl.when(s != 0)
        def _():
            for zz in range(ring):
                wait_block(m, c * ring + zz)
                for step in range(1, cores):
                    twin_copy(m, zz, step).start()
            for step in range(1, cores):
                other = lax.rem(c + step, cores)
                for zz in range(ring):
                    wait_block(m, other * ring + zz)

    def rs_copy(m, step):
        owner = lax.rem(j + step, owners)
        return remote(
            partial.at[m, owner],
            arrived.at[m, j],
            sem_rs_s.at[m, step - 1],
            sem_rs_r.at[m, j],
            place(s, owner),
        )

    def mix(m):
        x = [acts[m, k].astype(jnp.float32) for k in range(owners)]
        total = x[0] * x[0]
        for k in range(1, owners):
            total = total + x[k] * x[k]
        scale = lax.rsqrt(jnp.sum(total, axis=1, keepdims=True) / width + epsilon)
        normed = jnp.concatenate(
            [
                (x[k] * scale * gain_ref[:, k * block : (k + 1) * block]).astype(jnp.bfloat16)
                for k in range(owners)
            ],
            axis=1,
        )
        step_row = matmul(step_w[...], normed, NT_DIMS) + bias_col
        dt = jnp.maximum(step_row, 0.0) + jnp.log1p(jnp.exp(-jnp.abs(step_row)))
        a = dt * decay_col
        high = lax.Precision.HIGHEST
        fwd_row = matmul(a, tri_low, NT_DIMS, high)
        bwd_row = matmul(a, tri_up, NT_DIMS, high)
        fwd_col = matmul(tri_low, a, NT_DIMS, high)
        bwd_col = matmul(tri_up, a, NT_DIMS, high)
        value_raw = matmul(normed, value_w[...], NT_DIMS)
        write_raw = matmul(normed, write_w[...])
        read_raw = matmul(normed, read_w[...])
        gate_raw = matmul(normed, gate_w[...], NT_DIMS)
        pieces = inner // 128
        value = jnp.concatenate(
            [
                conv_act(
                    i,
                    value_raw[:, i * 128 : (i + 1) * 128],
                    [value_taps[k][:, i * 128 : (i + 1) * 128] for k in range(taps)],
                )
                for i in range(pieces)
            ],
            axis=1,
        )
        y = jnp.zeros((length, inner), jnp.float32)
        for g in range(groups):
            write = conv_act(
                pieces + 2 * g,
                write_raw[:, g * state : (g + 1) * state],
                [tap_w[k, g : g + 1, :] for k in range(taps)],
            )
            read = conv_act(
                pieces + 2 * g + 1,
                read_raw[:, g * state : (g + 1) * state],
                [tap_r[k, g : g + 1, :] for k in range(taps)],
            )
            scores = matmul(read, write, NT_DIMS)
            for e in range(per_group):
                h = g * per_group + e
                b = heads + h
                fwd_gap = fwd_col[:, h : h + 1] - fwd_row[h : h + 1, :]
                bwd_gap = bwd_col[:, b : b + 1] - bwd_row[b : b + 1, :]
                dt_f, dt_b = dt[h : h + 1, :], dt[b : b + 1, :]
                weight = jnp.exp(jnp.where(lower, fwd_gap, bwd_gap)) * jnp.where(
                    lower, dt_f, dt_b
                ) + jnp.where(diag, dt_b, 0.0)
                mixed = matmul((scores * weight).astype(jnp.bfloat16), value)
                y = jnp.where(lane_v // head == h, mixed, y)
        y = y + skip_row * value.astype(jnp.float32)
        gate = gate_raw.astype(jnp.bfloat16).astype(jnp.float32)
        gated = (y * silu(gate)).astype(jnp.bfloat16)
        sums = matmul(gated, out_w[...])
        for k in range(owners):
            partial[m, k] = sums[:, k * block : (k + 1) * block].astype(jnp.bfloat16)
        for step in range(1, owners):
            rs_copy(m, step).start()

    def hop_copy(m, zz):
        return remote(
            produced.at[m],
            acts.at[m, j],
            sem_hop_s.at[m, zz],
            sem_ag_r.at[m, j],
            {"pp": lax.rem(s + 1, sections), "fs": zz, "tp": c},
        )

    def fin_copy(m, p):
        return remote(
            leaving.at[m, p],
            final_in.at[m],
            sem_fin_s.at[m, p],
            sem_fin_r.at[m],
            {"pp": p, "fs": z, "tp": c},
        )

    def sq_copy(m, step):
        other = lax.rem(me + step, sections * owners)
        return remote(
            squares.at[m],
            square_in.at[m, j],
            sem_sq_s.at[m, step - 1],
            sem_sq_r.at[m, j],
            place(other // owners, lax.rem(other, owners)),
        )

    def reduce(m):
        total = partial[m, j].astype(jnp.float32)
        for step in range(1, owners):
            source = lax.rem(j + step, owners)
            remote(
                partial.at[m, source],
                arrived.at[m, source],
                sem_rs_s.at[m, 0],
                sem_rs_r.at[m, source],
                place(s, source),
            ).wait_recv()
            total = total + arrived[m, source].astype(jnp.float32)
        branch = total.astype(jnp.bfloat16).astype(jnp.float32)
        made = (acts[m, j].astype(jnp.float32) + 0.5 * branch).astype(jnp.bfloat16)

        @pl.when(s != last)
        def _():
            produced[m] = made
            for zz in range(ring):
                hop_copy(m, zz).start()

        @pl.when(s == last)
        def _():
            o = made.astype(jnp.float32)
            for p in range(sections):
                leaving[m, p] = o[p * share : (p + 1) * share].astype(jnp.bfloat16)
            col = jnp.sum(o * o, axis=1, keepdims=True)
            full = jnp.concatenate(
                [
                    jnp.broadcast_to(col, (length, 128)),
                    jnp.zeros((128 - length, 128), jnp.float32),
                ],
                axis=0,
            )
            row = jnp.transpose(full)[0:8, :]
            squares[m] = row
            square_in[m, j] = row
            for p in range(last):
                fin_copy(m, p).start()
            for step in range(1, sections * owners):
                sq_copy(m, step).start()
            pltpu.make_async_copy(leaving.at[m, last], final_in.at[m], sem_local.at[m]).start()

    def finish(m):
        @pl.when(s != last)
        def _():
            fin_copy(m, 0).wait_recv()

        @pl.when(s == last)
        def _():
            pltpu.make_async_copy(leaving.at[m, last], final_in.at[m], sem_local.at[m]).wait()

        for k in range(owners):

            @pl.when((s != last) | (j != k))
            def _():
                remote(
                    squares.at[m],
                    square_in.at[m, k],
                    sem_sq_s.at[m, 0],
                    sem_sq_r.at[m, k],
                    place(last, k),
                ).wait_recv()

        total = square_in[m, 0]
        for k in range(1, owners):
            total = total + square_in[m, k]
        scale = lax.rsqrt(total / width + epsilon)
        column[m] = jnp.transpose(jnp.broadcast_to(scale[0:1, :], (128, 128)))
        own = column[m, pl.ds(pl.multiple_of(s * share, 8), share), :]
        out_ref[m] = (final_in[m].astype(jnp.float32) * own).astype(jnp.bfloat16)

    for m in range(micro):
        receive(m)
        mix(m)
    for m in range(micro):
        reduce(m)
    for m in range(micro):
        finish(m)

    for m in range(micro):
        for step in range(1, owners):
            entry_copy(m, step).wait_send()
            rs_copy(m, step).wait_send()

        @pl.when(s != 0)
        def _():
            entry_copy(m, 0).wait_send()
            for zz in range(ring):
                for step in range(1, cores):
                    twin_copy(m, zz, step).wait_send()

        @pl.when(s != last)
        def _():
            for zz in range(ring):
                hop_copy(m, zz).wait_send()

        @pl.when(s == last)
        def _():
            for p in range(last):
                fin_copy(m, p).wait_send()
            for step in range(1, sections * owners):
                sq_copy(m, step).wait_send()


def fused_body(
    micro_in,
    norm_gain,
    proj_gate,
    proj_value,
    proj_write,
    proj_read,
    proj_step,
    step_bias,
    decay_log,
    skip_gain,
    conv_value,
    conv_write,
    conv_read,
    proj_out,
    sizes,
):
    sections, ring, cores = sizes["pp"], sizes["fs"], sizes["tp"]
    owners = ring * cores
    micro, share, block = micro_in.shape
    length = share * sections
    width = norm_gain.shape[1]
    taps = conv_value.shape[1]
    head = conv_value.shape[4]
    heads = conv_value.shape[2] * conv_value.shape[3]
    groups, state = conv_write.shape[2:]
    inner = heads * head
    args = (
        micro_in,
        norm_gain,
        jnp.transpose(proj_gate[0], (1, 2, 3, 0)).reshape(inner, width),
        jnp.transpose(proj_value[0], (1, 2, 3, 0)).reshape(inner, width),
        proj_write[0].reshape(width, groups * state),
        proj_read[0].reshape(width, groups * state),
        jnp.transpose(proj_step[0], (1, 2, 3, 0)).reshape(2 * heads, width),
        step_bias[0].reshape(2, heads),
        decay_log[0].reshape(2, heads),
        skip_gain[0].reshape(heads),
        conv_value[0].reshape(taps, heads, head),
        conv_write[0],
        conv_read[0],
        proj_out[0].reshape(inner, width),
    )
    vmem = pl.BlockSpec(memory_space=pltpu.VMEM)
    smem = pl.BlockSpec(memory_space=pltpu.SMEM)
    bf16, f32 = jnp.bfloat16, jnp.float32
    dma = pltpu.SemaphoreType.DMA
    pads = inner // 128 + 2 * groups
    return pl.pallas_call(
        functools.partial(relay_kernel, sizes),
        out_shape=jax.ShapeDtypeStruct(micro_in.shape, bf16),
        in_specs=[vmem] * 7 + [smem] * 3 + [vmem] * 4,
        out_specs=vmem,
        scratch_shapes=[
            pltpu.VMEM((micro, owners, sections, share, block), bf16),
            pltpu.VMEM((micro, owners, length, block), bf16),
            pltpu.VMEM((micro, owners, length, block), bf16),
            pltpu.VMEM((micro, owners, length, block), bf16),
            pltpu.VMEM((micro, length, block), bf16),
            pltpu.VMEM((micro, sections, share, block), bf16),
            pltpu.VMEM((micro, share, block), bf16),
            pltpu.VMEM((micro, 8, 128), f32),
            pltpu.VMEM((micro, owners, 8, 128), f32),
            pltpu.VMEM((micro, 128, 128), f32),
            pltpu.VMEM((pads, length + 16, 128), f32),
            dma((micro, owners)),
            dma((micro, owners, sections)),
            dma((micro, owners - 1)),
            dma((micro, owners)),
            dma((micro, ring)),
            dma((micro, owners)),
            dma((micro, ring, cores - 1)),
            dma((micro, sections)),
            dma((micro,)),
            dma((micro, sections * owners - 1)),
            dma((micro, owners)),
            dma((micro,)),
        ],
        compiler_params=pltpu.CompilerParams(collective_id=0, has_side_effects=True),
    )(*args)


def solution(mesh):
    sizes = dict(mesh.shape)

    def chosen(micro_in, *weights):
        fits = micro_in.shape[2] % 128 == 0 and micro_in.shape[1] % 8 == 0
        return (fused_body if fits else body)(micro_in, *weights, *(() if not fits else (sizes,)))

    return jax.shard_map(
        chosen,
        mesh=mesh,
        in_specs=(
            P(None, "pp", ("tp", "fs")),
            P("pp", None),
            P("pp", None, "tp", "fs", None),
            P("pp", None, "tp", "fs", None),
            P("pp", None, "tp", None),
            P("pp", None, "tp", None),
            P("pp", None, None, "tp", "fs"),
            P("pp", None, "tp", "fs"),
            P("pp", None, "tp", "fs"),
            P("pp", "tp", "fs"),
            P("pp", None, "tp", "fs", None),
            P("pp", None, "tp", None),
            P("pp", None, "tp", None),
            P("pp", "tp", "fs", None, None),
        ),
        out_specs=P(None, "pp", ("tp", "fs")),
        check_vma=False,
    )
```

```python
import functools

import jax
import jax.numpy as jnp
from jax import lax
from jax.experimental import pallas as pl
from jax.experimental.pallas import tpu as pltpu
from jax.sharding import PartitionSpec as P

epsilon = 1e-06


def own_rows_2(portion, span, axis):
    count = span * lax.axis_size(axis)
    sent = portion(jnp.int32(0), count).astype(jnp.bfloat16)
    return lax.psum_scatter(sent, axis, scatter_dimension=0, tiled=True).astype(jnp.float32)


def from_behind(block, axis, distance):
    devices = range(lax.axis_size(axis))
    route = [(i - distance, i) for i in devices if i - distance in devices]
    return lax.ppermute(block, axis, route)


def spread(value, axis, source):
    kept = jnp.where(lax.axis_index(axis) == source, value, 0).astype(value.dtype)
    return lax.psum(kept, axis)


def centred_conv(signal, conv_taps):
    span_width = conv_taps.shape[0]
    half_width = span_width // 2
    length = signal.shape[0]
    padded = jnp.pad(signal, ((half_width, half_width), (0, 0)))
    running = jnp.zeros_like(signal)
    for offset in range(span_width):
        running = running + padded[offset : offset + length] * conv_taps[offset]
    return running


def duality_mix(
    gate_flat,
    value_flat,
    write_flat,
    read_flat,
    step_raw,
    step_bias,
    decay_log,
    skip_gain,
    conv_value,
    conv_write,
    conv_read,
):
    groups, per_group = skip_gain.shape
    length = gate_flat.shape[0]
    head_size = value_flat.shape[1] // (groups * per_group)
    state_size = write_flat.shape[1] // groups
    taps_count = conv_value.shape[0]
    value_act = jax.nn.silu(
        centred_conv(value_flat.astype(jnp.float32), conv_value.reshape(taps_count, -1))
    ).astype(jnp.bfloat16)
    write_act = jax.nn.silu(
        centred_conv(write_flat.astype(jnp.float32), conv_write.reshape(taps_count, -1))
    ).astype(jnp.bfloat16)
    read_act = jax.nn.silu(
        centred_conv(read_flat.astype(jnp.float32), conv_read.reshape(taps_count, -1))
    ).astype(jnp.bfloat16)
    step_size = jax.nn.softplus(step_raw.reshape(length, 2, groups, per_group) + step_bias[None])
    log_decay = step_size * (-jnp.exp(decay_log))[None]
    fwd_cum = jnp.cumsum(log_decay[:, 0], axis=0)
    bwd_cum = jnp.flip(jnp.cumsum(jnp.flip(log_decay[:, 1], 0), axis=0), 0)
    positions = jnp.arange(length)
    lower_mask = (positions[:, None] >= positions[None, :])[:, :, None, None]
    upper_mask = (positions[:, None] <= positions[None, :])[:, :, None, None]
    fwd_weight = (
        jnp.exp(jnp.where(lower_mask, fwd_cum[:, None] - fwd_cum[None, :], -jnp.inf))
        * step_size[None, :, 0]
    )
    bwd_weight = (
        jnp.exp(jnp.where(upper_mask, bwd_cum[:, None] - bwd_cum[None, :], -jnp.inf))
        * step_size[None, :, 1]
    )
    scores = jnp.einsum(
        "tgn,sgn->tsg",
        read_act.reshape(length, groups, state_size),
        write_act.reshape(length, groups, state_size),
        preferred_element_type=jnp.float32,
    )
    combined = scores[:, :, :, None] * (fwd_weight + bwd_weight)
    value_heads = value_act.reshape(length, groups, per_group, head_size).astype(jnp.float32)
    mixed_heads = jnp.einsum(
        "tsgh,sghp->tghp", combined, value_heads, precision=lax.Precision.HIGHEST
    )
    mixed_heads = mixed_heads + skip_gain[None, :, :, None] * value_heads
    return (mixed_heads.reshape(length, -1) * jax.nn.silu(gate_flat.astype(jnp.float32))).astype(
        jnp.bfloat16
    )


def body(
    micro_in,
    norm_gain,
    proj_gate,
    proj_value,
    proj_write,
    proj_read,
    proj_step,
    step_bias,
    decay_log,
    skip_gain,
    conv_value,
    conv_write,
    conv_read,
    proj_out,
):
    section_count = lax.axis_size("pp")
    section_idx = lax.axis_index("pp")
    width_model = norm_gain.shape[1]
    fed_blocks = lax.all_gather(micro_in, "pp", axis=1, tiled=True)
    micro_count = fed_blocks.shape[0]
    length = fed_blocks.shape[1]
    fed_columns = jnp.swapaxes(fed_blocks, 1, 2)
    gain_vec = norm_gain[0].astype(jnp.float32)
    cut_gate = proj_gate.shape[2] * proj_gate.shape[3] * proj_gate.shape[4]
    cut_write = proj_write.shape[2] * proj_write.shape[3]
    weight_all = jnp.concatenate(
        [
            proj_gate[0].reshape(width_model, -1),
            proj_value[0].reshape(width_model, -1),
            proj_write[0].reshape(width_model, -1),
            proj_read[0].reshape(width_model, -1),
            proj_step[0].reshape(width_model, -1),
        ],
        axis=1,
    )
    out_weights = proj_out[0].reshape(-1, width_model)
    own_rows = width_model // lax.axis_size(("tp", "fs"))

    def project(column_block):
        gathered = lax.all_gather(column_block, ("tp", "fs"), axis=0, tiled=True)
        as_float = gathered.astype(jnp.float32)
        scale_rms = lax.rsqrt(jnp.mean(as_float * as_float, axis=0) + epsilon)
        normed = (as_float * scale_rms[None, :] * gain_vec[:, None]).astype(jnp.bfloat16)
        return lax.dot_general(
            normed, weight_all, (((0,), (0,)), ((), ())), preferred_element_type=jnp.float32
        )

    def term_maker(token_rows):

        def term_rows(offset, span_count):
            weight_cols = lax.dynamic_slice_in_dim(out_weights, offset, span_count, 1)
            return lax.dot_general(
                weight_cols,
                token_rows,
                (((0,), (1,)), ((), ())),
                preferred_element_type=jnp.float32,
            )

        return term_rows

    def mix_block(column_block):
        projected = project(column_block)
        gate_flat = projected[:, :cut_gate].astype(jnp.bfloat16)
        value_flat = projected[:, cut_gate : 2 * cut_gate].astype(jnp.bfloat16)
        write_flat = projected[:, 2 * cut_gate : 2 * cut_gate + cut_write].astype(jnp.bfloat16)
        read_flat = projected[:, 2 * cut_gate + cut_write : 2 * cut_gate + 2 * cut_write].astype(
            jnp.bfloat16
        )
        step_raw = projected[:, 2 * cut_gate + 2 * cut_write :]
        gated_out = duality_mix(
            gate_flat,
            value_flat,
            write_flat,
            read_flat,
            step_raw,
            step_bias[0],
            decay_log[0],
            skip_gain[0],
            conv_value[0],
            conv_write[0],
            conv_read[0],
        )
        summed = own_rows_2(term_maker(gated_out), own_rows, ("tp", "fs"))
        branch = lax.optimization_barrier(summed.astype(jnp.bfloat16))
        return (column_block.astype(jnp.float32) + 0.5 * branch.astype(jnp.float32)).astype(
            jnp.bfloat16
        )

    total_steps = micro_count + section_count - 1

    def advance(moment, loop_state):
        arriving, collected = loop_state
        pick_index = jnp.clip(moment, 0, micro_count - 1)
        fresh_block = lax.dynamic_index_in_dim(fed_columns, pick_index, 0, keepdims=False)
        current = jnp.where(section_idx == 0, fresh_block, arriving)
        produced = mix_block(current)
        slot_index = moment - section_idx
        keep_flag = (
            (section_idx == section_count - 1) & (slot_index >= 0) & (slot_index < micro_count)
        )
        slot_safe = jnp.clip(slot_index, 0, micro_count - 1)
        previous = lax.dynamic_index_in_dim(collected, slot_safe, 0, keepdims=False)
        collected = lax.dynamic_update_index_in_dim(
            collected, jnp.where(keep_flag, produced, previous), slot_safe, 0
        )
        arriving = from_behind(produced, "pp", 1)
        return (arriving, collected)

    start_loop = (jnp.zeros_like(fed_columns[0]), jnp.zeros_like(fed_columns))
    arriving, collected = lax.fori_loop(0, total_steps, advance, start_loop)
    shared = spread(collected, "pp", section_count - 1)
    token_share = length // section_count
    own_block = lax.dynamic_slice_in_dim(shared, section_idx * token_share, token_share, 2)
    as_float = own_block.astype(jnp.float32)
    partial_squares = jnp.sum(as_float * as_float, axis=1)
    total_squares = lax.psum(partial_squares, ("tp", "fs"))
    scale_rms = lax.rsqrt(total_squares / width_model + epsilon)
    result = (as_float * scale_rms[:, None, :]).astype(jnp.bfloat16)
    return jnp.swapaxes(result, 1, 2)


MESH = pl.DeviceIdType.MESH
NT_DIMS = (((1,), (1,)), ((), ()))
NN_DIMS = (((1,), (0,)), ((), ()))


def silu(x):
    return 0.5 * x * (1.0 + jnp.tanh(0.5 * x))


def matmul(left, right, dims=NN_DIMS, precision=None):
    return lax.dot_general(
        left, right, dims, precision=precision, preferred_element_type=jnp.float32
    )


def relay_kernel(
    sizes,
    in_ref,
    gain_ref,
    gate_hbm,
    value_hbm,
    write_hbm,
    read_hbm,
    step_w,
    bias_ref,
    decay_ref,
    skip_ref,
    tap_v,
    tap_w,
    tap_r,
    out_hbm,
    out_ref,
    gate_w,
    value_w,
    raw_w,
    mixed_w,
    out_w,
    entry,
    acts,
    partial,
    from_twin,
    own_sum,
    pair_sum,
    arrived,
    produced,
    leaving,
    final_in,
    squares,
    square_in,
    column,
    padded,
    sem_load,
    sem_entry_s,
    sem_entry_r,
    sem_pre_s,
    sem_pre_r,
    sem_rs_s,
    sem_rs_r,
    sem_hop_s,
    sem_ag_r,
    sem_twin_s,
    sem_fin_s,
    sem_fin_r,
    sem_sq_s,
    sem_sq_r,
    sem_local,
):
    sections, ring, cores = sizes["pp"], sizes["fs"], sizes["tp"]
    owners = ring * cores
    micro, share, block = in_ref.shape
    length = share * sections
    width = owners * block
    inner = gate_w.shape[0]
    groups, state = tap_w.shape[1], tap_w.shape[2]
    taps, heads, head = tap_v.shape
    per_group = heads // groups
    half = taps // 2
    s = lax.axis_index("pp")
    z = lax.axis_index("fs")
    c = lax.axis_index("tp")
    j = c * ring + z
    last = sections - 1
    me = s * owners + j

    def place(section, owner):
        return {"pp": section, "fs": lax.rem(owner, ring), "tp": owner // ring}

    loads = [
        pltpu.make_async_copy(src, dst, sem_load.at[i])
        for i, (src, dst) in enumerate(
            (
                (write_hbm, raw_w.at[0]),
                (read_hbm, raw_w.at[1]),
                (value_hbm, value_w),
                (gate_hbm, gate_w),
                (out_hbm, out_w),
            )
        )
    ]
    for load in loads:
        load.start()
    far_first = sorted(range(1, ring), key=lambda k: -min(k, ring - k))

    barrier = pltpu.get_barrier_semaphore()
    for step in range(1, sections * owners):
        other = lax.rem(me + step, sections * owners)
        pl.semaphore_signal(
            barrier,
            inc=1,
            device_id=place(other // owners, lax.rem(other, owners)),
            device_id_type=MESH,
        )
    pl.semaphore_wait(barrier, sections * owners - 1)

    def remote(src, dst, send_sem, recv_sem, target):
        return pltpu.make_async_remote_copy(
            src_ref=src,
            dst_ref=dst,
            send_sem=send_sem,
            recv_sem=recv_sem,
            device_id=target,
            device_id_type=MESH,
        )

    def entry_copy(m, step):
        return remote(
            in_ref.at[m],
            entry.at[m, z, s],
            sem_entry_s.at[m, step],
            sem_entry_r.at[m, z, s],
            {"pp": 0, "fs": lax.rem(z + step, ring), "tp": c},
        )

    def entry_own(m):
        return pltpu.make_async_copy(in_ref.at[m], entry.at[m, z, s], sem_entry_r.at[m, z, s])

    for m in range(micro):
        for step in far_first:
            entry_copy(m, step).start()

        @pl.when(s == 0)
        def _():
            entry_own(m).start()

        @pl.when(s != 0)
        def _():
            entry_copy(m, 0).start()

    lane_v = lax.broadcasted_iota(jnp.int32, (1, heads * head), 1)
    row8 = lax.broadcasted_iota(jnp.int32, (2 * heads, 1), 0)
    bias_col = jnp.zeros((2 * heads, 1), jnp.float32)
    decay_col = jnp.zeros((2 * heads, 1), jnp.float32)
    skip_row = jnp.zeros((1, heads * head), jnp.float32)
    for i in range(2 * heads):
        d, h = i // heads, i % heads
        bias_col = jnp.where(row8 == i, bias_ref[d, h], bias_col)
        decay_col = jnp.where(row8 == i, decay_ref[d, h], decay_col)
    for h in range(heads):
        skip_row = jnp.where(lane_v // head == h, skip_ref[h], skip_row)
    decay_col = -jnp.exp(decay_col)
    value_taps = [
        jnp.concatenate([tap_v[k, h : h + 1, :] for h in range(heads)], axis=1)
        for k in range(taps)
    ]
    tpos = lax.broadcasted_iota(jnp.int32, (length, length), 0)
    spos = lax.broadcasted_iota(jnp.int32, (length, length), 1)
    lower = spos <= tpos
    diag = spos == tpos
    tri_low = jnp.where(lower, 1.0, 0.0)
    tri_up = jnp.where(spos >= tpos, 1.0, 0.0)
    edge = jnp.zeros((8, 128), jnp.float32)
    for q in range(padded.shape[0]):
        padded[q, 0:8, :] = edge
        padded[q, 8 + length : 16 + length, :] = edge

    for load in loads:
        load.wait()
    chunk = 256
    rows_per = chunk // groups
    to_row = lax.broadcasted_iota(jnp.int32, (chunk, chunk), 0)
    from_row = lax.broadcasted_iota(jnp.int32, (chunk, chunk), 1)
    order = jnp.where(
        from_row == lax.rem(to_row, rows_per) * groups + to_row // rows_per, 1.0, 0.0
    ).astype(jnp.bfloat16)
    for i in range(2):
        for b in range(width // rows_per):
            sorted_rows = matmul(order, raw_w[i, b * chunk : (b + 1) * chunk, :]).astype(
                jnp.bfloat16
            )
            for g in range(groups):
                mixed_w[
                    i, b * rows_per : (b + 1) * rows_per, g * state : (g + 1) * state
                ] = sorted_rows[g * rows_per : (g + 1) * rows_per]

    def conv_act(slot, signal, rows):
        padded[slot, 8 : 8 + length, :] = signal.astype(jnp.bfloat16).astype(jnp.float32)
        start = 8 - half
        total = padded[slot, start : start + length, :] * rows[0]
        for k in range(1, taps):
            total = total + padded[slot, start + k : start + k + length, :] * rows[k]
        return silu(total).astype(jnp.bfloat16)

    def twin_copy(m, zz, step):
        slot = c * ring + zz
        other = lax.rem(c + step, cores)
        return remote(
            acts.at[m, slot],
            acts.at[m, slot],
            sem_twin_s.at[m, zz, step - 1],
            sem_ag_r.at[m, slot],
            {"pp": s, "fs": z, "tp": other},
        )

    def wait_block(m, slot):
        remote(
            acts.at[m, slot],
            acts.at[m, slot],
            sem_twin_s.at[m, 0, 0],
            sem_ag_r.at[m, slot],
            place(s, slot),
        ).wait_recv()

    def receive(m):
        for step in range(ring):
            zz = lax.rem(z + step, ring)
            slot = c * ring + zz

            @pl.when(s == 0)
            def _():
                for p in range(sections):
                    pltpu.make_async_copy(
                        in_ref.at[m], entry.at[m, zz, p], sem_entry_r.at[m, zz, p]
                    ).wait()
                acts[m, slot] = jnp.concatenate(
                    [entry[m, zz, p].astype(jnp.float32) for p in range(sections)], axis=0
                ).astype(jnp.bfloat16)

            @pl.when(s != 0)
            def _():
                wait_block(m, slot)

            for twin in range(1, cores):
                twin_copy(m, zz, twin).start()
        for twin in range(1, cores):
            other = lax.rem(c + twin, cores)
            for step in range(ring):
                wait_block(m, other * ring + lax.rem(z + step, ring))

    def pre_copy(m, twin, zz):
        other = lax.rem(c + twin, cores)
        return remote(
            partial.at[m, twin - 1, zz],
            from_twin.at[m, twin - 1, zz],
            sem_pre_s.at[m, twin - 1, zz],
            sem_pre_r.at[m, twin - 1, zz],
            {"pp": s, "fs": z, "tp": other},
        )

    def rs_copy(m, step):
        zz = lax.rem(z + step, ring)
        return remote(
            pair_sum.at[m, zz],
            arrived.at[m, z],
            sem_rs_s.at[m, step - 1],
            sem_rs_r.at[m, z],
            {"pp": s, "fs": zz, "tp": c},
        )

    def mix(m):
        x = [acts[m, k].astype(jnp.float32) for k in range(owners)]
        total = x[0] * x[0]
        for k in range(1, owners):
            total = total + x[k] * x[k]
        scale = lax.rsqrt(jnp.sum(total, axis=1, keepdims=True) / width + epsilon)
        normed = jnp.concatenate(
            [
                (x[k] * scale * gain_ref[:, k * block : (k + 1) * block]).astype(jnp.bfloat16)
                for k in range(owners)
            ],
            axis=1,
        )
        step_row = (
            jnp.concatenate([matmul(step_w[d], normed, NT_DIMS) for d in range(2)], axis=0)
            + bias_col
        )
        dt = jnp.maximum(step_row, 0.0) + jnp.log1p(jnp.exp(-jnp.abs(step_row)))
        a = dt * decay_col
        high = lax.Precision.HIGHEST
        fwd_row = matmul(a, tri_low, NT_DIMS, high)
        bwd_row = matmul(a, tri_up, NT_DIMS, high)
        fwd_col = matmul(tri_low, a, NT_DIMS, high)
        bwd_col = matmul(tri_up, a, NT_DIMS, high)
        value_raw = matmul(normed, value_w[...], NT_DIMS)
        write_raw = matmul(normed, mixed_w[0])
        read_raw = matmul(normed, mixed_w[1])
        gate_raw = matmul(normed, gate_w[...], NT_DIMS)
        pieces = inner // 128
        value = jnp.concatenate(
            [
                conv_act(
                    i,
                    value_raw[:, i * 128 : (i + 1) * 128],
                    [value_taps[k][:, i * 128 : (i + 1) * 128] for k in range(taps)],
                )
                for i in range(pieces)
            ],
            axis=1,
        )
        y = jnp.zeros((length, inner), jnp.float32)
        for g in range(groups):
            write = conv_act(
                pieces + 2 * g,
                write_raw[:, g * state : (g + 1) * state],
                [tap_w[k, g : g + 1, :] for k in range(taps)],
            )
            read = conv_act(
                pieces + 2 * g + 1,
                read_raw[:, g * state : (g + 1) * state],
                [tap_r[k, g : g + 1, :] for k in range(taps)],
            )
            scores = matmul(read, write, NT_DIMS)
            for e in range(per_group):
                h = g * per_group + e
                b = heads + h
                fwd_gap = fwd_col[:, h : h + 1] - fwd_row[h : h + 1, :]
                bwd_gap = bwd_col[:, b : b + 1] - bwd_row[b : b + 1, :]
                dt_f, dt_b = dt[h : h + 1, :], dt[b : b + 1, :]
                weight = jnp.exp(jnp.where(lower, fwd_gap, bwd_gap)) * jnp.where(
                    lower, dt_f, dt_b
                ) + jnp.where(diag, dt_b, 0.0)
                mixed = matmul((scores * weight).astype(jnp.bfloat16), value)
                y = jnp.where(lane_v // head == h, mixed, y)
        y = y + skip_row * value.astype(jnp.float32)
        gate = gate_raw.astype(jnp.bfloat16).astype(jnp.float32)
        gated = (y * silu(gate)).astype(jnp.bfloat16)
        span = ring * block

        def half_sums(core):
            start = pl.multiple_of(core * span, 128)
            return matmul(gated, out_w[:, pl.ds(start, span)])

        for twin in range(1, cores):
            sums = half_sums(lax.rem(c + twin, cores))
            for zz in range(ring):
                partial[m, twin - 1, zz] = sums[:, zz * block : (zz + 1) * block].astype(
                    jnp.bfloat16
                )
                pre_copy(m, twin, zz).start()
        sums = half_sums(c)
        for zz in range(ring):
            own_sum[m, zz] = sums[:, zz * block : (zz + 1) * block]

    def pair(m, zz):
        total = own_sum[m, zz]
        for twin in range(1, cores):
            pre_copy(m, twin, zz).wait_recv()
            total = total + from_twin[m, twin - 1, zz].astype(jnp.float32)
        return total

    def send_pairs(m):
        for step in far_first:
            zz = lax.rem(z + step, ring)
            pair_sum[m, zz] = pair(m, zz).astype(jnp.bfloat16)
            rs_copy(m, step).start()
        own_sum[m, z] = pair(m, z)

    def hop_copy(m, step):
        return remote(
            produced.at[m],
            acts.at[m, j],
            sem_hop_s.at[m, step],
            sem_ag_r.at[m, j],
            {"pp": lax.rem(s + 1, sections), "fs": lax.rem(z + step, ring), "tp": c},
        )

    def fin_copy(m, p):
        return remote(
            leaving.at[m, p],
            final_in.at[m],
            sem_fin_s.at[m, p],
            sem_fin_r.at[m],
            {"pp": p, "fs": z, "tp": c},
        )

    def sq_copy(m, step):
        other = lax.rem(me + step, sections * owners)
        return remote(
            squares.at[m],
            square_in.at[m, j],
            sem_sq_s.at[m, step - 1],
            sem_sq_r.at[m, j],
            place(other // owners, lax.rem(other, owners)),
        )

    def reduce(m):
        total = own_sum[m, z]
        for step in range(1, ring):
            source = lax.rem(z + step, ring)
            remote(
                pair_sum.at[m, source],
                arrived.at[m, source],
                sem_rs_s.at[m, step - 1],
                sem_rs_r.at[m, source],
                {"pp": s, "fs": source, "tp": c},
            ).wait_recv()
            total = total + arrived[m, source].astype(jnp.float32)
        branch = total.astype(jnp.bfloat16).astype(jnp.float32)
        made = (acts[m, j].astype(jnp.float32) + 0.5 * branch).astype(jnp.bfloat16)

        @pl.when(s != last)
        def _():
            produced[m] = made
            for step in (*far_first, 0):
                hop_copy(m, step).start()

        @pl.when(s == last)
        def _():
            o = made.astype(jnp.float32)
            for p in range(sections):
                leaving[m, p] = o[p * share : (p + 1) * share].astype(jnp.bfloat16)
            col = jnp.sum(o * o, axis=1, keepdims=True)
            full = jnp.concatenate(
                [
                    jnp.broadcast_to(col, (length, 128)),
                    jnp.zeros((128 - length, 128), jnp.float32),
                ],
                axis=0,
            )
            row = jnp.transpose(full)[0:1, :]
            squares[m] = row
            square_in[m, j] = row
            for p in range(last):
                fin_copy(m, p).start()
            for step in range(1, sections * owners):
                sq_copy(m, step).start()
            pltpu.make_async_copy(leaving.at[m, last], final_in.at[m], sem_local.at[m]).start()

    def finish(m):
        @pl.when(s != last)
        def _():
            fin_copy(m, 0).wait_recv()

        @pl.when(s == last)
        def _():
            pltpu.make_async_copy(leaving.at[m, last], final_in.at[m], sem_local.at[m]).wait()

        for k in range(owners):

            @pl.when((s != last) | (j != k))
            def _():
                remote(
                    squares.at[m],
                    square_in.at[m, k],
                    sem_sq_s.at[m, 0],
                    sem_sq_r.at[m, k],
                    place(last, k),
                ).wait_recv()

        total = square_in[m, 0]
        for k in range(1, owners):
            total = total + square_in[m, k]
        scale = lax.rsqrt(total / width + epsilon)
        column[m] = jnp.transpose(jnp.broadcast_to(scale, (128, 128)))
        own = column[m, pl.ds(pl.multiple_of(s * share, 8), share), :]
        out_ref[m] = (final_in[m].astype(jnp.float32) * own).astype(jnp.bfloat16)

    for m in range(micro):
        receive(m)
        mix(m)
        send_pairs(m)
    for m in range(micro):
        reduce(m)
    for m in range(micro):
        finish(m)

    for m in range(micro):
        for step in range(1, ring):
            entry_copy(m, step).wait_send()
            rs_copy(m, step).wait_send()
        for twin in range(1, cores):
            for zz in range(ring):
                pre_copy(m, twin, zz).wait_send()
                twin_copy(m, zz, twin).wait_send()

        @pl.when(s != 0)
        def _():
            entry_copy(m, 0).wait_send()

        @pl.when(s != last)
        def _():
            for zz in range(ring):
                hop_copy(m, zz).wait_send()

        @pl.when(s == last)
        def _():
            for p in range(last):
                fin_copy(m, p).wait_send()
            for step in range(1, sections * owners):
                sq_copy(m, step).wait_send()


def fused_body(
    micro_in,
    norm_gain,
    proj_gate,
    proj_value,
    proj_write,
    proj_read,
    proj_step,
    step_bias,
    decay_log,
    skip_gain,
    conv_value,
    conv_write,
    conv_read,
    proj_out,
    sizes,
):
    sections, ring, cores = sizes["pp"], sizes["fs"], sizes["tp"]
    owners = ring * cores
    micro, share, block = micro_in.shape
    length = share * sections
    width = norm_gain.shape[1]
    taps = conv_value.shape[1]
    head = conv_value.shape[4]
    heads = conv_value.shape[2] * conv_value.shape[3]
    groups, state = conv_write.shape[2:]
    inner = heads * head
    args = (
        micro_in,
        norm_gain,
        jnp.transpose(proj_gate[0], (1, 2, 3, 0)).reshape(inner, width),
        jnp.transpose(proj_value[0], (1, 2, 3, 0)).reshape(inner, width),
        proj_write[0].reshape(width * groups, state),
        proj_read[0].reshape(width * groups, state),
        jnp.transpose(proj_step[0], (1, 2, 3, 0)).reshape(2, heads, width),
        step_bias[0].reshape(2, heads),
        decay_log[0].reshape(2, heads),
        skip_gain[0].reshape(heads),
        conv_value[0].reshape(taps, heads, head),
        conv_write[0],
        conv_read[0],
        proj_out[0].reshape(inner, width),
    )
    vmem = pl.BlockSpec(memory_space=pltpu.VMEM)
    smem = pl.BlockSpec(memory_space=pltpu.SMEM)
    whole = pl.BlockSpec(memory_space=pl.ANY)
    bf16, f32 = jnp.bfloat16, jnp.float32
    dma = pltpu.SemaphoreType.DMA
    pads = inner // 128 + 2 * groups
    return pl.pallas_call(
        functools.partial(relay_kernel, sizes),
        out_shape=jax.ShapeDtypeStruct(micro_in.shape, bf16),
        in_specs=[vmem] * 2 + [whole] * 4 + [vmem] + [smem] * 3 + [vmem] * 3 + [whole],
        out_specs=vmem,
        scratch_shapes=[
            pltpu.VMEM((inner, width), bf16),
            pltpu.VMEM((inner, width), bf16),
            pltpu.VMEM((2, width * groups, state), bf16),
            pltpu.VMEM((2, width, groups * state), bf16),
            pltpu.VMEM((inner, width), bf16),
            pltpu.VMEM((micro, ring, sections, share, block), bf16),
            pltpu.VMEM((micro, owners, length, block), bf16),
            pltpu.VMEM((micro, cores - 1, ring, length, block), bf16),
            pltpu.VMEM((micro, cores - 1, ring, length, block), bf16),
            pltpu.VMEM((micro, ring, length, block), f32),
            pltpu.VMEM((micro, ring, length, block), bf16),
            pltpu.VMEM((micro, ring, length, block), bf16),
            pltpu.VMEM((micro, length, block), bf16),
            pltpu.VMEM((micro, sections, share, block), bf16),
            pltpu.VMEM((micro, share, block), bf16),
            pltpu.VMEM((micro, 1, 128), f32),
            pltpu.VMEM((micro, owners, 1, 128), f32),
            pltpu.VMEM((micro, 128, 128), f32),
            pltpu.VMEM((pads, length + 16, 128), f32),
            dma((5,)),
            dma((micro, ring)),
            dma((micro, ring, sections)),
            dma((micro, cores - 1, ring)),
            dma((micro, cores - 1, ring)),
            dma((micro, ring - 1)),
            dma((micro, ring)),
            dma((micro, ring)),
            dma((micro, owners)),
            dma((micro, ring, cores - 1)),
            dma((micro, sections)),
            dma((micro,)),
            dma((micro, sections * owners - 1)),
            dma((micro, owners)),
            dma((micro,)),
        ],
        compiler_params=pltpu.CompilerParams(collective_id=0, has_side_effects=True),
    )(*args)


def solution(mesh):
    sizes = dict(mesh.shape)

    def chosen(micro_in, *weights):
        fits = micro_in.shape[2] % 128 == 0 and micro_in.shape[1] % 8 == 0 and 256 % weights[3].shape[2] == 0 and weights[3].shape[3] == 128
        return (fused_body if fits else body)(micro_in, *weights, *(() if not fits else (sizes,)))

    return jax.shard_map(
        chosen,
        mesh=mesh,
        in_specs=(
            P(None, "pp", ("tp", "fs")),
            P("pp", None),
            P("pp", None, "tp", "fs", None),
            P("pp", None, "tp", "fs", None),
            P("pp", None, "tp", None),
            P("pp", None, "tp", None),
            P("pp", None, None, "tp", "fs"),
            P("pp", None, "tp", "fs"),
            P("pp", None, "tp", "fs"),
            P("pp", "tp", "fs"),
            P("pp", None, "tp", "fs", None),
            P("pp", None, "tp", None),
            P("pp", None, "tp", None),
            P("pp", "tp", "fs", None, None),
        ),
        out_specs=P(None, "pp", ("tp", "fs")),
        check_vma=False,
    )
```

```python
import functools

import jax
import jax.numpy as jnp
from jax import lax
from jax.experimental import pallas as pl
from jax.experimental.pallas import tpu as pltpu
from jax.sharding import PartitionSpec as P

epsilon = 1e-06


def own_rows_2(portion, span, axis):
    count = span * lax.axis_size(axis)
    sent = portion(jnp.int32(0), count).astype(jnp.bfloat16)
    return lax.psum_scatter(sent, axis, scatter_dimension=0, tiled=True).astype(jnp.float32)


def from_behind(block, axis, distance):
    devices = range(lax.axis_size(axis))
    route = [(i - distance, i) for i in devices if i - distance in devices]
    return lax.ppermute(block, axis, route)


def spread(value, axis, source):
    kept = jnp.where(lax.axis_index(axis) == source, value, 0).astype(value.dtype)
    return lax.psum(kept, axis)


def centred_conv(signal, conv_taps):
    span_width = conv_taps.shape[0]
    half_width = span_width // 2
    length = signal.shape[0]
    padded = jnp.pad(signal, ((half_width, half_width), (0, 0)))
    running = jnp.zeros_like(signal)
    for offset in range(span_width):
        running = running + padded[offset : offset + length] * conv_taps[offset]
    return running


def duality_mix(
    gate_flat,
    value_flat,
    write_flat,
    read_flat,
    step_raw,
    step_bias,
    decay_log,
    skip_gain,
    conv_value,
    conv_write,
    conv_read,
):
    groups, per_group = skip_gain.shape
    length = gate_flat.shape[0]
    head_size = value_flat.shape[1] // (groups * per_group)
    state_size = write_flat.shape[1] // groups
    taps_count = conv_value.shape[0]
    value_act = jax.nn.silu(
        centred_conv(value_flat.astype(jnp.float32), conv_value.reshape(taps_count, -1))
    ).astype(jnp.bfloat16)
    write_act = jax.nn.silu(
        centred_conv(write_flat.astype(jnp.float32), conv_write.reshape(taps_count, -1))
    ).astype(jnp.bfloat16)
    read_act = jax.nn.silu(
        centred_conv(read_flat.astype(jnp.float32), conv_read.reshape(taps_count, -1))
    ).astype(jnp.bfloat16)
    step_size = jax.nn.softplus(step_raw.reshape(length, 2, groups, per_group) + step_bias[None])
    log_decay = step_size * (-jnp.exp(decay_log))[None]
    fwd_cum = jnp.cumsum(log_decay[:, 0], axis=0)
    bwd_cum = jnp.flip(jnp.cumsum(jnp.flip(log_decay[:, 1], 0), axis=0), 0)
    positions = jnp.arange(length)
    lower_mask = (positions[:, None] >= positions[None, :])[:, :, None, None]
    upper_mask = (positions[:, None] <= positions[None, :])[:, :, None, None]
    fwd_weight = (
        jnp.exp(jnp.where(lower_mask, fwd_cum[:, None] - fwd_cum[None, :], -jnp.inf))
        * step_size[None, :, 0]
    )
    bwd_weight = (
        jnp.exp(jnp.where(upper_mask, bwd_cum[:, None] - bwd_cum[None, :], -jnp.inf))
        * step_size[None, :, 1]
    )
    scores = jnp.einsum(
        "tgn,sgn->tsg",
        read_act.reshape(length, groups, state_size),
        write_act.reshape(length, groups, state_size),
        preferred_element_type=jnp.float32,
    )
    combined = scores[:, :, :, None] * (fwd_weight + bwd_weight)
    value_heads = value_act.reshape(length, groups, per_group, head_size).astype(jnp.float32)
    mixed_heads = jnp.einsum(
        "tsgh,sghp->tghp", combined, value_heads, precision=lax.Precision.HIGHEST
    )
    mixed_heads = mixed_heads + skip_gain[None, :, :, None] * value_heads
    return (mixed_heads.reshape(length, -1) * jax.nn.silu(gate_flat.astype(jnp.float32))).astype(
        jnp.bfloat16
    )


def body(
    micro_in,
    norm_gain,
    proj_gate,
    proj_value,
    proj_write,
    proj_read,
    proj_step,
    step_bias,
    decay_log,
    skip_gain,
    conv_value,
    conv_write,
    conv_read,
    proj_out,
):
    section_count = lax.axis_size("pp")
    section_idx = lax.axis_index("pp")
    width_model = norm_gain.shape[1]
    fed_blocks = lax.all_gather(micro_in, "pp", axis=1, tiled=True)
    micro_count = fed_blocks.shape[0]
    length = fed_blocks.shape[1]
    fed_columns = jnp.swapaxes(fed_blocks, 1, 2)
    gain_vec = norm_gain[0].astype(jnp.float32)
    cut_gate = proj_gate.shape[2] * proj_gate.shape[3] * proj_gate.shape[4]
    cut_write = proj_write.shape[2] * proj_write.shape[3]
    weight_all = jnp.concatenate(
        [
            proj_gate[0].reshape(width_model, -1),
            proj_value[0].reshape(width_model, -1),
            proj_write[0].reshape(width_model, -1),
            proj_read[0].reshape(width_model, -1),
            proj_step[0].reshape(width_model, -1),
        ],
        axis=1,
    )
    out_weights = proj_out[0].reshape(-1, width_model)
    own_rows = width_model // lax.axis_size(("tp", "fs"))

    def project(column_block):
        gathered = lax.all_gather(column_block, ("tp", "fs"), axis=0, tiled=True)
        as_float = gathered.astype(jnp.float32)
        scale_rms = lax.rsqrt(jnp.mean(as_float * as_float, axis=0) + epsilon)
        normed = (as_float * scale_rms[None, :] * gain_vec[:, None]).astype(jnp.bfloat16)
        return lax.dot_general(
            normed, weight_all, (((0,), (0,)), ((), ())), preferred_element_type=jnp.float32
        )

    def term_maker(token_rows):

        def term_rows(offset, span_count):
            weight_cols = lax.dynamic_slice_in_dim(out_weights, offset, span_count, 1)
            return lax.dot_general(
                weight_cols,
                token_rows,
                (((0,), (1,)), ((), ())),
                preferred_element_type=jnp.float32,
            )

        return term_rows

    def mix_block(column_block):
        projected = project(column_block)
        gate_flat = projected[:, :cut_gate].astype(jnp.bfloat16)
        value_flat = projected[:, cut_gate : 2 * cut_gate].astype(jnp.bfloat16)
        write_flat = projected[:, 2 * cut_gate : 2 * cut_gate + cut_write].astype(jnp.bfloat16)
        read_flat = projected[:, 2 * cut_gate + cut_write : 2 * cut_gate + 2 * cut_write].astype(
            jnp.bfloat16
        )
        step_raw = projected[:, 2 * cut_gate + 2 * cut_write :]
        gated_out = duality_mix(
            gate_flat,
            value_flat,
            write_flat,
            read_flat,
            step_raw,
            step_bias[0],
            decay_log[0],
            skip_gain[0],
            conv_value[0],
            conv_write[0],
            conv_read[0],
        )
        summed = own_rows_2(term_maker(gated_out), own_rows, ("tp", "fs"))
        branch = lax.optimization_barrier(summed.astype(jnp.bfloat16))
        return (column_block.astype(jnp.float32) + 0.5 * branch.astype(jnp.float32)).astype(
            jnp.bfloat16
        )

    total_steps = micro_count + section_count - 1

    def advance(moment, loop_state):
        arriving, collected = loop_state
        pick_index = jnp.clip(moment, 0, micro_count - 1)
        fresh_block = lax.dynamic_index_in_dim(fed_columns, pick_index, 0, keepdims=False)
        current = jnp.where(section_idx == 0, fresh_block, arriving)
        produced = mix_block(current)
        slot_index = moment - section_idx
        keep_flag = (
            (section_idx == section_count - 1) & (slot_index >= 0) & (slot_index < micro_count)
        )
        slot_safe = jnp.clip(slot_index, 0, micro_count - 1)
        previous = lax.dynamic_index_in_dim(collected, slot_safe, 0, keepdims=False)
        collected = lax.dynamic_update_index_in_dim(
            collected, jnp.where(keep_flag, produced, previous), slot_safe, 0
        )
        arriving = from_behind(produced, "pp", 1)
        return (arriving, collected)

    start_loop = (jnp.zeros_like(fed_columns[0]), jnp.zeros_like(fed_columns))
    arriving, collected = lax.fori_loop(0, total_steps, advance, start_loop)
    shared = spread(collected, "pp", section_count - 1)
    token_share = length // section_count
    own_block = lax.dynamic_slice_in_dim(shared, section_idx * token_share, token_share, 2)
    as_float = own_block.astype(jnp.float32)
    partial_squares = jnp.sum(as_float * as_float, axis=1)
    total_squares = lax.psum(partial_squares, ("tp", "fs"))
    scale_rms = lax.rsqrt(total_squares / width_model + epsilon)
    result = (as_float * scale_rms[:, None, :]).astype(jnp.bfloat16)
    return jnp.swapaxes(result, 1, 2)


MESH = pl.DeviceIdType.MESH
NT_DIMS = (((1,), (1,)), ((), ()))
NN_DIMS = (((1,), (0,)), ((), ()))


def silu(x):
    return 0.5 * x * (1.0 + jnp.tanh(0.5 * x))


def matmul(left, right, dims=NN_DIMS, precision=None):
    return lax.dot_general(
        left, right, dims, precision=precision, preferred_element_type=jnp.float32
    )


def relay_kernel(
    sizes,
    in_ref,
    gain_ref,
    gate_hbm,
    value_hbm,
    write_hbm,
    read_hbm,
    step_w,
    bias_ref,
    decay_ref,
    skip_ref,
    tap_v,
    tap_w,
    tap_r,
    out_hbm,
    out_ref,
    gate_w,
    value_w,
    raw_w,
    mixed_w,
    out_w,
    entry,
    acts,
    partial,
    from_twin,
    own_sum,
    pair_sum,
    arrived,
    produced,
    leaving,
    final_in,
    squares,
    square_in,
    column,
    padded,
    sem_load,
    sem_entry_s,
    sem_entry_r,
    sem_pre_s,
    sem_pre_r,
    sem_rs_s,
    sem_rs_r,
    sem_hop_s,
    sem_ag_r,
    sem_twin_s,
    sem_fin_s,
    sem_fin_r,
    sem_sq_s,
    sem_sq_r,
    sem_local,
):
    sections, ring, cores = sizes["pp"], sizes["fs"], sizes["tp"]
    owners = ring * cores
    micro, share, block = in_ref.shape
    length = share * sections
    width = owners * block
    inner = gate_w.shape[0]
    groups, state = tap_w.shape[1], tap_w.shape[2]
    taps, heads, head = tap_v.shape
    per_group = heads // groups
    half = taps // 2
    s = lax.axis_index("pp")
    z = lax.axis_index("fs")
    c = lax.axis_index("tp")
    j = c * ring + z
    last = sections - 1
    me = s * owners + j

    def place(section, owner):
        return {"pp": section, "fs": lax.rem(owner, ring), "tp": owner // ring}

    loads = [
        pltpu.make_async_copy(src, dst, sem_load.at[i])
        for i, (src, dst) in enumerate(
            (
                (write_hbm, raw_w.at[0]),
                (read_hbm, raw_w.at[1]),
                (value_hbm, value_w),
                (gate_hbm, gate_w),
                (out_hbm, out_w),
            )
        )
    ]
    for load in loads:
        load.start()
    far_first = sorted(range(1, ring), key=lambda k: -min(k, ring - k))

    barrier = pltpu.get_barrier_semaphore()
    for step in range(1, sections * owners):
        other = lax.rem(me + step, sections * owners)
        pl.semaphore_signal(
            barrier,
            inc=1,
            device_id=place(other // owners, lax.rem(other, owners)),
            device_id_type=MESH,
        )
    pl.semaphore_wait(barrier, sections * owners - 1)

    def remote(src, dst, send_sem, recv_sem, target):
        return pltpu.make_async_remote_copy(
            src_ref=src,
            dst_ref=dst,
            send_sem=send_sem,
            recv_sem=recv_sem,
            device_id=target,
            device_id_type=MESH,
        )

    def entry_copy(m, step):
        return remote(
            in_ref.at[m],
            entry.at[m, z, s],
            sem_entry_s.at[m, step],
            sem_entry_r.at[m, z, s],
            {"pp": 0, "fs": lax.rem(z + step, ring), "tp": c},
        )

    def entry_own(m):
        return pltpu.make_async_copy(in_ref.at[m], entry.at[m, z, s], sem_entry_r.at[m, z, s])

    for m in range(micro):
        for step in far_first:
            entry_copy(m, step).start()

        @pl.when(s == 0)
        def _():
            entry_own(m).start()

        @pl.when(s != 0)
        def _():
            entry_copy(m, 0).start()

    lane_v = lax.broadcasted_iota(jnp.int32, (1, heads * head), 1)
    row8 = lax.broadcasted_iota(jnp.int32, (2 * heads, 1), 0)
    bias_col = jnp.zeros((2 * heads, 1), jnp.float32)
    decay_col = jnp.zeros((2 * heads, 1), jnp.float32)
    skip_row = jnp.zeros((1, heads * head), jnp.float32)
    for i in range(2 * heads):
        d, h = i // heads, i % heads
        bias_col = jnp.where(row8 == i, bias_ref[d, h], bias_col)
        decay_col = jnp.where(row8 == i, decay_ref[d, h], decay_col)
    for h in range(heads):
        skip_row = jnp.where(lane_v // head == h, skip_ref[h], skip_row)
    decay_col = -jnp.exp(decay_col)
    value_taps = [
        jnp.concatenate([tap_v[k, h : h + 1, :] for h in range(heads)], axis=1)
        for k in range(taps)
    ]
    tpos = lax.broadcasted_iota(jnp.int32, (length, length), 0)
    spos = lax.broadcasted_iota(jnp.int32, (length, length), 1)
    lower = spos <= tpos
    diag = spos == tpos
    tri_low = jnp.where(lower, 1.0, 0.0)
    tri_up = jnp.where(spos >= tpos, 1.0, 0.0)
    edge = jnp.zeros((8, 128), jnp.float32)
    for q in range(padded.shape[0]):
        padded[q, 0:8, :] = edge
        padded[q, 8 + length : 16 + length, :] = edge

    for load in loads:
        load.wait()
    chunk = 256
    rows_per = chunk // groups
    to_row = lax.broadcasted_iota(jnp.int32, (chunk, chunk), 0)
    from_row = lax.broadcasted_iota(jnp.int32, (chunk, chunk), 1)
    order = jnp.where(
        from_row == lax.rem(to_row, rows_per) * groups + to_row // rows_per, 1.0, 0.0
    ).astype(jnp.bfloat16)
    for i in range(2):
        for b in range(width // rows_per):
            sorted_rows = matmul(order, raw_w[i, b * chunk : (b + 1) * chunk, :]).astype(
                jnp.bfloat16
            )
            for g in range(groups):
                mixed_w[
                    i, b * rows_per : (b + 1) * rows_per, g * state : (g + 1) * state
                ] = sorted_rows[g * rows_per : (g + 1) * rows_per]

    def conv_act(slot, signal, rows):
        padded[slot, 8 : 8 + length, :] = signal.astype(jnp.bfloat16).astype(jnp.float32)
        start = 8 - half
        total = padded[slot, start : start + length, :] * rows[0]
        for k in range(1, taps):
            total = total + padded[slot, start + k : start + k + length, :] * rows[k]
        return silu(total).astype(jnp.bfloat16)

    def twin_copy(m, zz, step):
        slot = c * ring + zz
        other = lax.rem(c + step, cores)
        return remote(
            acts.at[m, slot],
            acts.at[m, slot],
            sem_twin_s.at[m, zz, step - 1],
            sem_ag_r.at[m, slot],
            {"pp": s, "fs": z, "tp": other},
        )

    def wait_block(m, slot):
        remote(
            acts.at[m, slot],
            acts.at[m, slot],
            sem_twin_s.at[m, 0, 0],
            sem_ag_r.at[m, slot],
            place(s, slot),
        ).wait_recv()

    def receive(m):
        for step in range(ring):
            zz = lax.rem(z + step, ring)
            slot = c * ring + zz

            @pl.when(s == 0)
            def _():
                for p in range(sections):
                    pltpu.make_async_copy(
                        in_ref.at[m], entry.at[m, zz, p], sem_entry_r.at[m, zz, p]
                    ).wait()
                acts[m, slot] = jnp.concatenate(
                    [entry[m, zz, p].astype(jnp.float32) for p in range(sections)], axis=0
                ).astype(jnp.bfloat16)

            @pl.when(s != 0)
            def _():
                wait_block(m, slot)

            for twin in range(1, cores):
                twin_copy(m, zz, twin).start()
        for twin in range(1, cores):
            other = lax.rem(c + twin, cores)
            for step in range(ring):
                wait_block(m, other * ring + lax.rem(z + step, ring))

    def pre_copy(m, twin, zz):
        other = lax.rem(c + twin, cores)
        return remote(
            partial.at[m, twin - 1, zz],
            from_twin.at[m, twin - 1, zz],
            sem_pre_s.at[m, twin - 1, zz],
            sem_pre_r.at[m, twin - 1, zz],
            {"pp": s, "fs": z, "tp": other},
        )

    def rs_copy(m, step):
        zz = lax.rem(z + step, ring)
        return remote(
            pair_sum.at[m, zz],
            arrived.at[m, z],
            sem_rs_s.at[m, step - 1],
            sem_rs_r.at[m, z],
            {"pp": s, "fs": zz, "tp": c},
        )

    def mix(m):
        x = [acts[m, k].astype(jnp.float32) for k in range(owners)]
        total = x[0] * x[0]
        for k in range(1, owners):
            total = total + x[k] * x[k]
        scale = lax.rsqrt(jnp.sum(total, axis=1, keepdims=True) / width + epsilon)
        normed = jnp.concatenate(
            [
                (x[k] * scale * gain_ref[:, k * block : (k + 1) * block]).astype(jnp.bfloat16)
                for k in range(owners)
            ],
            axis=1,
        )
        step_row = (
            jnp.concatenate([matmul(step_w[d], normed, NT_DIMS) for d in range(2)], axis=0)
            + bias_col
        )
        dt = jnp.maximum(step_row, 0.0) + jnp.log1p(jnp.exp(-jnp.abs(step_row)))
        a = dt * decay_col
        high = lax.Precision.HIGHEST
        fwd_row = matmul(a, tri_low, NT_DIMS, high)
        bwd_row = matmul(a, tri_up, NT_DIMS, high)
        fwd_col = matmul(tri_low, a, NT_DIMS, high)
        bwd_col = matmul(tri_up, a, NT_DIMS, high)
        value_raw = matmul(normed, value_w[...], NT_DIMS)
        write_raw = matmul(normed, mixed_w[0])
        read_raw = matmul(normed, mixed_w[1])
        gate_raw = matmul(normed, gate_w[...], NT_DIMS)
        pieces = inner // 128
        value = jnp.concatenate(
            [
                conv_act(
                    i,
                    value_raw[:, i * 128 : (i + 1) * 128],
                    [value_taps[k][:, i * 128 : (i + 1) * 128] for k in range(taps)],
                )
                for i in range(pieces)
            ],
            axis=1,
        )
        y = jnp.zeros((length, inner), jnp.float32)
        for g in range(groups):
            write = conv_act(
                pieces + 2 * g,
                write_raw[:, g * state : (g + 1) * state],
                [tap_w[k, g : g + 1, :] for k in range(taps)],
            )
            read = conv_act(
                pieces + 2 * g + 1,
                read_raw[:, g * state : (g + 1) * state],
                [tap_r[k, g : g + 1, :] for k in range(taps)],
            )
            scores = matmul(read, write, NT_DIMS)
            for e in range(per_group):
                h = g * per_group + e
                b = heads + h
                fwd_gap = fwd_col[:, h : h + 1] - fwd_row[h : h + 1, :]
                bwd_gap = bwd_col[:, b : b + 1] - bwd_row[b : b + 1, :]
                dt_f, dt_b = dt[h : h + 1, :], dt[b : b + 1, :]
                weight = jnp.exp(jnp.where(lower, fwd_gap, bwd_gap)) * jnp.where(
                    lower, dt_f, dt_b
                ) + jnp.where(diag, dt_b, 0.0)
                mixed = matmul((scores * weight).astype(jnp.bfloat16), value)
                y = jnp.where(lane_v // head == h, mixed, y)
        y = y + skip_row * value.astype(jnp.float32)
        gate = gate_raw.astype(jnp.bfloat16).astype(jnp.float32)
        gated = (y * silu(gate)).astype(jnp.bfloat16)
        span = ring * block

        def half_sums(core):
            start = pl.multiple_of(core * span, 128)
            return matmul(gated, out_w[:, pl.ds(start, span)])

        for twin in range(1, cores):
            sums = half_sums(lax.rem(c + twin, cores))
            for zz in range(ring):
                partial[m, twin - 1, zz] = sums[:, zz * block : (zz + 1) * block].astype(
                    jnp.bfloat16
                )
                pre_copy(m, twin, zz).start()
        sums = half_sums(c)
        for zz in range(ring):
            own_sum[m, zz] = sums[:, zz * block : (zz + 1) * block]

    def pair(m, zz):
        total = own_sum[m, zz]
        for twin in range(1, cores):
            pre_copy(m, twin, zz).wait_recv()
            total = total + from_twin[m, twin - 1, zz].astype(jnp.float32)
        return total

    def send_pairs(m):
        for step in far_first:
            zz = lax.rem(z + step, ring)
            pair_sum[m, zz] = pair(m, zz).astype(jnp.bfloat16)
            rs_copy(m, step).start()
        own_sum[m, z] = pair(m, z)

    def hop_copy(m, step):
        return remote(
            produced.at[m],
            acts.at[m, j],
            sem_hop_s.at[m, step],
            sem_ag_r.at[m, j],
            {"pp": lax.rem(s + 1, sections), "fs": lax.rem(z + step, ring), "tp": c},
        )

    def fin_copy(m, p):
        return remote(
            leaving.at[m, p],
            final_in.at[m],
            sem_fin_s.at[m, p],
            sem_fin_r.at[m],
            {"pp": p, "fs": z, "tp": c},
        )

    def sq_copy(m, step):
        other = lax.rem(me + step, sections * owners)
        return remote(
            squares.at[m],
            square_in.at[m, j],
            sem_sq_s.at[m, step - 1],
            sem_sq_r.at[m, j],
            place(other // owners, lax.rem(other, owners)),
        )

    def reduce(m):
        total = own_sum[m, z]
        for step in range(1, ring):
            source = lax.rem(z + step, ring)
            remote(
                pair_sum.at[m, source],
                arrived.at[m, source],
                sem_rs_s.at[m, step - 1],
                sem_rs_r.at[m, source],
                {"pp": s, "fs": source, "tp": c},
            ).wait_recv()
            total = total + arrived[m, source].astype(jnp.float32)
        branch = total.astype(jnp.bfloat16).astype(jnp.float32)
        made = (acts[m, j].astype(jnp.float32) + 0.5 * branch).astype(jnp.bfloat16)

        @pl.when(s != last)
        def _():
            produced[m] = made
            for step in (*far_first, 0):
                hop_copy(m, step).start()

        @pl.when(s == last)
        def _():
            o = made.astype(jnp.float32)
            for p in range(sections):
                leaving[m, p] = o[p * share : (p + 1) * share].astype(jnp.bfloat16)
            col = jnp.sum(o * o, axis=1, keepdims=True)
            full = jnp.concatenate(
                [
                    jnp.broadcast_to(col, (length, 128)),
                    jnp.zeros((128 - length, 128), jnp.float32),
                ],
                axis=0,
            )
            row = jnp.transpose(full)[0:1, :]
            squares[m] = row
            square_in[m, j] = row
            for p in range(last):
                fin_copy(m, p).start()
            for step in range(1, sections * owners):
                sq_copy(m, step).start()
            pltpu.make_async_copy(leaving.at[m, last], final_in.at[m], sem_local.at[m]).start()

    def finish(m):
        @pl.when(s != last)
        def _():
            fin_copy(m, 0).wait_recv()

        @pl.when(s == last)
        def _():
            pltpu.make_async_copy(leaving.at[m, last], final_in.at[m], sem_local.at[m]).wait()

        for k in range(owners):

            @pl.when((s != last) | (j != k))
            def _():
                remote(
                    squares.at[m],
                    square_in.at[m, k],
                    sem_sq_s.at[m, 0],
                    sem_sq_r.at[m, k],
                    place(last, k),
                ).wait_recv()

        total = square_in[m, 0]
        for k in range(1, owners):
            total = total + square_in[m, k]
        scale = lax.rsqrt(total / width + epsilon)
        column[m] = jnp.transpose(jnp.broadcast_to(scale, (128, 128)))
        own = column[m, pl.ds(pl.multiple_of(s * share, 8), share), :]
        out_ref[m] = (final_in[m].astype(jnp.float32) * own).astype(jnp.bfloat16)

    receive(0)
    mix(0)
    send_pairs(0)
    for m in range(1, micro):
        receive(m)
        mix(m)
        reduce(m - 1)
        send_pairs(m)
    reduce(micro - 1)
    for m in range(micro):
        finish(m)

    for m in range(micro):
        for step in range(1, ring):
            entry_copy(m, step).wait_send()
            rs_copy(m, step).wait_send()
        for twin in range(1, cores):
            for zz in range(ring):
                pre_copy(m, twin, zz).wait_send()
                twin_copy(m, zz, twin).wait_send()

        @pl.when(s != 0)
        def _():
            entry_copy(m, 0).wait_send()

        @pl.when(s != last)
        def _():
            for zz in range(ring):
                hop_copy(m, zz).wait_send()

        @pl.when(s == last)
        def _():
            for p in range(last):
                fin_copy(m, p).wait_send()
            for step in range(1, sections * owners):
                sq_copy(m, step).wait_send()


def fused_body(
    micro_in,
    norm_gain,
    proj_gate,
    proj_value,
    proj_write,
    proj_read,
    proj_step,
    step_bias,
    decay_log,
    skip_gain,
    conv_value,
    conv_write,
    conv_read,
    proj_out,
    sizes,
):
    sections, ring, cores = sizes["pp"], sizes["fs"], sizes["tp"]
    owners = ring * cores
    micro, share, block = micro_in.shape
    length = share * sections
    width = norm_gain.shape[1]
    taps = conv_value.shape[1]
    head = conv_value.shape[4]
    heads = conv_value.shape[2] * conv_value.shape[3]
    groups, state = conv_write.shape[2:]
    inner = heads * head
    args = (
        micro_in,
        norm_gain,
        jnp.transpose(proj_gate[0], (1, 2, 3, 0)).reshape(inner, width),
        jnp.transpose(proj_value[0], (1, 2, 3, 0)).reshape(inner, width),
        proj_write[0].reshape(width * groups, state),
        proj_read[0].reshape(width * groups, state),
        jnp.transpose(proj_step[0], (1, 2, 3, 0)).reshape(2, heads, width),
        step_bias[0].reshape(2, heads),
        decay_log[0].reshape(2, heads),
        skip_gain[0].reshape(heads),
        conv_value[0].reshape(taps, heads, head),
        conv_write[0],
        conv_read[0],
        proj_out[0].reshape(inner, width),
    )
    vmem = pl.BlockSpec(memory_space=pltpu.VMEM)
    smem = pl.BlockSpec(memory_space=pltpu.SMEM)
    whole = pl.BlockSpec(memory_space=pl.ANY)
    bf16, f32 = jnp.bfloat16, jnp.float32
    dma = pltpu.SemaphoreType.DMA
    pads = inner // 128 + 2 * groups
    return pl.pallas_call(
        functools.partial(relay_kernel, sizes),
        out_shape=jax.ShapeDtypeStruct(micro_in.shape, bf16),
        in_specs=[vmem] * 2 + [whole] * 4 + [vmem] + [smem] * 3 + [vmem] * 3 + [whole],
        out_specs=vmem,
        scratch_shapes=[
            pltpu.VMEM((inner, width), bf16),
            pltpu.VMEM((inner, width), bf16),
            pltpu.VMEM((2, width * groups, state), bf16),
            pltpu.VMEM((2, width, groups * state), bf16),
            pltpu.VMEM((inner, width), bf16),
            pltpu.VMEM((micro, ring, sections, share, block), bf16),
            pltpu.VMEM((micro, owners, length, block), bf16),
            pltpu.VMEM((micro, cores - 1, ring, length, block), bf16),
            pltpu.VMEM((micro, cores - 1, ring, length, block), bf16),
            pltpu.VMEM((micro, ring, length, block), f32),
            pltpu.VMEM((micro, ring, length, block), bf16),
            pltpu.VMEM((micro, ring, length, block), bf16),
            pltpu.VMEM((micro, length, block), bf16),
            pltpu.VMEM((micro, sections, share, block), bf16),
            pltpu.VMEM((micro, share, block), bf16),
            pltpu.VMEM((micro, 1, 128), f32),
            pltpu.VMEM((micro, owners, 1, 128), f32),
            pltpu.VMEM((micro, 128, 128), f32),
            pltpu.VMEM((pads, length + 16, 128), f32),
            dma((5,)),
            dma((micro, ring)),
            dma((micro, ring, sections)),
            dma((micro, cores - 1, ring)),
            dma((micro, cores - 1, ring)),
            dma((micro, ring - 1)),
            dma((micro, ring)),
            dma((micro, ring)),
            dma((micro, owners)),
            dma((micro, ring, cores - 1)),
            dma((micro, sections)),
            dma((micro,)),
            dma((micro, sections * owners - 1)),
            dma((micro, owners)),
            dma((micro,)),
        ],
        compiler_params=pltpu.CompilerParams(collective_id=0, has_side_effects=True),
    )(*args)


def solution(mesh):
    sizes = dict(mesh.shape)

    def chosen(micro_in, *weights):
        fits = micro_in.shape[2] % 128 == 0 and micro_in.shape[1] % 8 == 0 and 256 % weights[3].shape[2] == 0 and weights[3].shape[3] == 128
        return (fused_body if fits else body)(micro_in, *weights, *(() if not fits else (sizes,)))

    return jax.shard_map(
        chosen,
        mesh=mesh,
        in_specs=(
            P(None, "pp", ("tp", "fs")),
            P("pp", None),
            P("pp", None, "tp", "fs", None),
            P("pp", None, "tp", "fs", None),
            P("pp", None, "tp", None),
            P("pp", None, "tp", None),
            P("pp", None, None, "tp", "fs"),
            P("pp", None, "tp", "fs"),
            P("pp", None, "tp", "fs"),
            P("pp", "tp", "fs"),
            P("pp", None, "tp", "fs", None),
            P("pp", None, "tp", None),
            P("pp", None, "tp", None),
            P("pp", "tp", "fs", None, None),
        ),
        out_specs=P(None, "pp", ("tp", "fs")),
        check_vma=False,
    )
```

```python
import functools

import jax
import jax.numpy as jnp
from jax import lax
from jax.experimental import pallas as pl
from jax.experimental.pallas import tpu as pltpu
from jax.sharding import PartitionSpec as P

epsilon = 1e-06


def own_rows_2(portion, span, axis):
    count = span * lax.axis_size(axis)
    sent = portion(jnp.int32(0), count).astype(jnp.bfloat16)
    return lax.psum_scatter(sent, axis, scatter_dimension=0, tiled=True).astype(jnp.float32)


def from_behind(block, axis, distance):
    devices = range(lax.axis_size(axis))
    route = [(i - distance, i) for i in devices if i - distance in devices]
    return lax.ppermute(block, axis, route)


def spread(value, axis, source):
    kept = jnp.where(lax.axis_index(axis) == source, value, 0).astype(value.dtype)
    return lax.psum(kept, axis)


def centred_conv(signal, conv_taps):
    span_width = conv_taps.shape[0]
    half_width = span_width // 2
    length = signal.shape[0]
    padded = jnp.pad(signal, ((half_width, half_width), (0, 0)))
    running = jnp.zeros_like(signal)
    for offset in range(span_width):
        running = running + padded[offset : offset + length] * conv_taps[offset]
    return running


def duality_mix(
    gate_flat,
    value_flat,
    write_flat,
    read_flat,
    step_raw,
    step_bias,
    decay_log,
    skip_gain,
    conv_value,
    conv_write,
    conv_read,
):
    groups, per_group = skip_gain.shape
    length = gate_flat.shape[0]
    head_size = value_flat.shape[1] // (groups * per_group)
    state_size = write_flat.shape[1] // groups
    taps_count = conv_value.shape[0]
    value_act = jax.nn.silu(
        centred_conv(value_flat.astype(jnp.float32), conv_value.reshape(taps_count, -1))
    ).astype(jnp.bfloat16)
    write_act = jax.nn.silu(
        centred_conv(write_flat.astype(jnp.float32), conv_write.reshape(taps_count, -1))
    ).astype(jnp.bfloat16)
    read_act = jax.nn.silu(
        centred_conv(read_flat.astype(jnp.float32), conv_read.reshape(taps_count, -1))
    ).astype(jnp.bfloat16)
    step_size = jax.nn.softplus(step_raw.reshape(length, 2, groups, per_group) + step_bias[None])
    log_decay = step_size * (-jnp.exp(decay_log))[None]
    fwd_cum = jnp.cumsum(log_decay[:, 0], axis=0)
    bwd_cum = jnp.flip(jnp.cumsum(jnp.flip(log_decay[:, 1], 0), axis=0), 0)
    positions = jnp.arange(length)
    lower_mask = (positions[:, None] >= positions[None, :])[:, :, None, None]
    upper_mask = (positions[:, None] <= positions[None, :])[:, :, None, None]
    fwd_weight = (
        jnp.exp(jnp.where(lower_mask, fwd_cum[:, None] - fwd_cum[None, :], -jnp.inf))
        * step_size[None, :, 0]
    )
    bwd_weight = (
        jnp.exp(jnp.where(upper_mask, bwd_cum[:, None] - bwd_cum[None, :], -jnp.inf))
        * step_size[None, :, 1]
    )
    scores = jnp.einsum(
        "tgn,sgn->tsg",
        read_act.reshape(length, groups, state_size),
        write_act.reshape(length, groups, state_size),
        preferred_element_type=jnp.float32,
    )
    combined = scores[:, :, :, None] * (fwd_weight + bwd_weight)
    value_heads = value_act.reshape(length, groups, per_group, head_size).astype(jnp.float32)
    mixed_heads = jnp.einsum(
        "tsgh,sghp->tghp", combined, value_heads, precision=lax.Precision.HIGHEST
    )
    mixed_heads = mixed_heads + skip_gain[None, :, :, None] * value_heads
    return (mixed_heads.reshape(length, -1) * jax.nn.silu(gate_flat.astype(jnp.float32))).astype(
        jnp.bfloat16
    )


def body(
    micro_in,
    norm_gain,
    proj_gate,
    proj_value,
    proj_write,
    proj_read,
    proj_step,
    step_bias,
    decay_log,
    skip_gain,
    conv_value,
    conv_write,
    conv_read,
    proj_out,
):
    section_count = lax.axis_size("pp")
    section_idx = lax.axis_index("pp")
    width_model = norm_gain.shape[1]
    fed_blocks = lax.all_gather(micro_in, "pp", axis=1, tiled=True)
    micro_count = fed_blocks.shape[0]
    length = fed_blocks.shape[1]
    fed_columns = jnp.swapaxes(fed_blocks, 1, 2)
    gain_vec = norm_gain[0].astype(jnp.float32)
    cut_gate = proj_gate.shape[2] * proj_gate.shape[3] * proj_gate.shape[4]
    cut_write = proj_write.shape[2] * proj_write.shape[3]
    weight_all = jnp.concatenate(
        [
            proj_gate[0].reshape(width_model, -1),
            proj_value[0].reshape(width_model, -1),
            proj_write[0].reshape(width_model, -1),
            proj_read[0].reshape(width_model, -1),
            proj_step[0].reshape(width_model, -1),
        ],
        axis=1,
    )
    out_weights = proj_out[0].reshape(-1, width_model)
    own_rows = width_model // lax.axis_size(("tp", "fs"))

    def project(column_block):
        gathered = lax.all_gather(column_block, ("tp", "fs"), axis=0, tiled=True)
        as_float = gathered.astype(jnp.float32)
        scale_rms = lax.rsqrt(jnp.mean(as_float * as_float, axis=0) + epsilon)
        normed = (as_float * scale_rms[None, :] * gain_vec[:, None]).astype(jnp.bfloat16)
        return lax.dot_general(
            normed, weight_all, (((0,), (0,)), ((), ())), preferred_element_type=jnp.float32
        )

    def term_maker(token_rows):

        def term_rows(offset, span_count):
            weight_cols = lax.dynamic_slice_in_dim(out_weights, offset, span_count, 1)
            return lax.dot_general(
                weight_cols,
                token_rows,
                (((0,), (1,)), ((), ())),
                preferred_element_type=jnp.float32,
            )

        return term_rows

    def mix_block(column_block):
        projected = project(column_block)
        gate_flat = projected[:, :cut_gate].astype(jnp.bfloat16)
        value_flat = projected[:, cut_gate : 2 * cut_gate].astype(jnp.bfloat16)
        write_flat = projected[:, 2 * cut_gate : 2 * cut_gate + cut_write].astype(jnp.bfloat16)
        read_flat = projected[:, 2 * cut_gate + cut_write : 2 * cut_gate + 2 * cut_write].astype(
            jnp.bfloat16
        )
        step_raw = projected[:, 2 * cut_gate + 2 * cut_write :]
        gated_out = duality_mix(
            gate_flat,
            value_flat,
            write_flat,
            read_flat,
            step_raw,
            step_bias[0],
            decay_log[0],
            skip_gain[0],
            conv_value[0],
            conv_write[0],
            conv_read[0],
        )
        summed = own_rows_2(term_maker(gated_out), own_rows, ("tp", "fs"))
        branch = lax.optimization_barrier(summed.astype(jnp.bfloat16))
        return (column_block.astype(jnp.float32) + 0.5 * branch.astype(jnp.float32)).astype(
            jnp.bfloat16
        )

    total_steps = micro_count + section_count - 1

    def advance(moment, loop_state):
        arriving, collected = loop_state
        pick_index = jnp.clip(moment, 0, micro_count - 1)
        fresh_block = lax.dynamic_index_in_dim(fed_columns, pick_index, 0, keepdims=False)
        current = jnp.where(section_idx == 0, fresh_block, arriving)
        produced = mix_block(current)
        slot_index = moment - section_idx
        keep_flag = (
            (section_idx == section_count - 1) & (slot_index >= 0) & (slot_index < micro_count)
        )
        slot_safe = jnp.clip(slot_index, 0, micro_count - 1)
        previous = lax.dynamic_index_in_dim(collected, slot_safe, 0, keepdims=False)
        collected = lax.dynamic_update_index_in_dim(
            collected, jnp.where(keep_flag, produced, previous), slot_safe, 0
        )
        arriving = from_behind(produced, "pp", 1)
        return (arriving, collected)

    start_loop = (jnp.zeros_like(fed_columns[0]), jnp.zeros_like(fed_columns))
    arriving, collected = lax.fori_loop(0, total_steps, advance, start_loop)
    shared = spread(collected, "pp", section_count - 1)
    token_share = length // section_count
    own_block = lax.dynamic_slice_in_dim(shared, section_idx * token_share, token_share, 2)
    as_float = own_block.astype(jnp.float32)
    partial_squares = jnp.sum(as_float * as_float, axis=1)
    total_squares = lax.psum(partial_squares, ("tp", "fs"))
    scale_rms = lax.rsqrt(total_squares / width_model + epsilon)
    result = (as_float * scale_rms[:, None, :]).astype(jnp.bfloat16)
    return jnp.swapaxes(result, 1, 2)


MESH = pl.DeviceIdType.MESH
NT_DIMS = (((1,), (1,)), ((), ()))
NN_DIMS = (((1,), (0,)), ((), ()))


def silu(x):
    return 0.5 * x * (1.0 + jnp.tanh(0.5 * x))


def matmul(left, right, dims=NN_DIMS, precision=None):
    return lax.dot_general(
        left, right, dims, precision=precision, preferred_element_type=jnp.float32
    )


def relay_kernel(
    sizes,
    in_ref,
    gain_ref,
    gate_hbm,
    value_hbm,
    write_hbm,
    read_hbm,
    step_w,
    bias_ref,
    decay_ref,
    skip_ref,
    tap_v,
    tap_w,
    tap_r,
    out_hbm,
    out_ref,
    gate_w,
    value_w,
    raw_w,
    mixed_w,
    out_w,
    entry,
    acts,
    partial,
    from_twin,
    own_sum,
    pair_sum,
    arrived,
    produced,
    leaving,
    final_in,
    squares,
    square_in,
    column,
    padded,
    sem_load,
    sem_entry_s,
    sem_entry_r,
    sem_pre_s,
    sem_pre_r,
    sem_rs_s,
    sem_rs_r,
    sem_hop_s,
    sem_ag_r,
    sem_twin_s,
    sem_fin_s,
    sem_fin_r,
    sem_sq_s,
    sem_sq_r,
    sem_local,
):
    sections, ring, cores = sizes["pp"], sizes["fs"], sizes["tp"]
    owners = ring * cores
    micro, share, block = in_ref.shape
    length = share * sections
    width = owners * block
    inner = gate_w.shape[0]
    groups, state = tap_w.shape[1], tap_w.shape[2]
    taps, heads, head = tap_v.shape
    per_group = heads // groups
    half = taps // 2
    s = lax.axis_index("pp")
    z = lax.axis_index("fs")
    c = lax.axis_index("tp")
    j = c * ring + z
    last = sections - 1
    me = s * owners + j

    def place(section, owner):
        return {"pp": section, "fs": lax.rem(owner, ring), "tp": owner // ring}

    loads = [
        pltpu.make_async_copy(src, dst, sem_load.at[i])
        for i, (src, dst) in enumerate(
            (
                (write_hbm, raw_w.at[0]),
                (read_hbm, raw_w.at[1]),
                (value_hbm, value_w),
                (gate_hbm, gate_w),
                (out_hbm, out_w),
            )
        )
    ]
    for load in loads:
        load.start()
    far_first = sorted(range(1, ring), key=lambda k: -min(k, ring - k))

    barrier = pltpu.get_barrier_semaphore()
    for step in range(1, sections * owners):
        other = lax.rem(me + step, sections * owners)
        pl.semaphore_signal(
            barrier,
            inc=1,
            device_id=place(other // owners, lax.rem(other, owners)),
            device_id_type=MESH,
        )
    pl.semaphore_wait(barrier, sections * owners - 1)

    def remote(src, dst, send_sem, recv_sem, target):
        return pltpu.make_async_remote_copy(
            src_ref=src,
            dst_ref=dst,
            send_sem=send_sem,
            recv_sem=recv_sem,
            device_id=target,
            device_id_type=MESH,
        )

    def entry_copy(m, step):
        return remote(
            in_ref.at[m],
            entry.at[m, z, s],
            sem_entry_s.at[m, step],
            sem_entry_r.at[m, z, s],
            {"pp": 0, "fs": lax.rem(z + step, ring), "tp": c},
        )

    def entry_own(m):
        return pltpu.make_async_copy(in_ref.at[m], entry.at[m, z, s], sem_entry_r.at[m, z, s])

    for m in range(micro):
        for step in far_first:
            entry_copy(m, step).start()

        @pl.when(s == 0)
        def _():
            entry_own(m).start()

        @pl.when(s != 0)
        def _():
            entry_copy(m, 0).start()

    lane_v = lax.broadcasted_iota(jnp.int32, (1, heads * head), 1)
    row8 = lax.broadcasted_iota(jnp.int32, (2 * heads, 1), 0)
    bias_col = jnp.zeros((2 * heads, 1), jnp.float32)
    decay_col = jnp.zeros((2 * heads, 1), jnp.float32)
    skip_row = jnp.zeros((1, heads * head), jnp.float32)
    for i in range(2 * heads):
        d, h = i // heads, i % heads
        bias_col = jnp.where(row8 == i, bias_ref[d, h], bias_col)
        decay_col = jnp.where(row8 == i, decay_ref[d, h], decay_col)
    for h in range(heads):
        skip_row = jnp.where(lane_v // head == h, skip_ref[h], skip_row)
    decay_col = -jnp.exp(decay_col)
    value_taps = [
        jnp.concatenate([tap_v[k, h : h + 1, :] for h in range(heads)], axis=1)
        for k in range(taps)
    ]
    tpos = lax.broadcasted_iota(jnp.int32, (length, length), 0)
    spos = lax.broadcasted_iota(jnp.int32, (length, length), 1)
    lower = spos <= tpos
    diag = spos == tpos
    tri_low = jnp.where(lower, 1.0, 0.0)
    tri_up = jnp.where(spos >= tpos, 1.0, 0.0)
    edge = jnp.zeros((8, 128), jnp.float32)
    for q in range(padded.shape[0]):
        padded[q, 0:8, :] = edge
        padded[q, 8 + length : 16 + length, :] = edge

    for load in loads:
        load.wait()
    chunk = 256
    rows_per = chunk // groups
    to_row = lax.broadcasted_iota(jnp.int32, (chunk, chunk), 0)
    from_row = lax.broadcasted_iota(jnp.int32, (chunk, chunk), 1)
    order = jnp.where(
        from_row == lax.rem(to_row, rows_per) * groups + to_row // rows_per, 1.0, 0.0
    ).astype(jnp.bfloat16)
    for i in range(2):
        for b in range(width // rows_per):
            sorted_rows = matmul(order, raw_w[i, b * chunk : (b + 1) * chunk, :]).astype(
                jnp.bfloat16
            )
            for g in range(groups):
                mixed_w[
                    i, b * rows_per : (b + 1) * rows_per, g * state : (g + 1) * state
                ] = sorted_rows[g * rows_per : (g + 1) * rows_per]

    def conv_act(slot, signal, rows):
        padded[slot, 8 : 8 + length, :] = signal.astype(jnp.bfloat16).astype(jnp.float32)
        start = 8 - half
        total = padded[slot, start : start + length, :] * rows[0]
        for k in range(1, taps):
            total = total + padded[slot, start + k : start + k + length, :] * rows[k]
        return silu(total).astype(jnp.bfloat16)

    def twin_copy(m, zz, step):
        slot = c * ring + zz
        other = lax.rem(c + step, cores)
        return remote(
            acts.at[m, slot],
            acts.at[m, slot],
            sem_twin_s.at[m, zz, step - 1],
            sem_ag_r.at[m, slot],
            {"pp": s, "fs": z, "tp": other},
        )

    def wait_block(m, slot):
        remote(
            acts.at[m, slot],
            acts.at[m, slot],
            sem_twin_s.at[m, 0, 0],
            sem_ag_r.at[m, slot],
            place(s, slot),
        ).wait_recv()

    def receive(m):
        for step in range(ring):
            zz = lax.rem(z + step, ring)
            slot = c * ring + zz

            @pl.when(s == 0)
            def _():
                for p in range(sections):
                    pltpu.make_async_copy(
                        in_ref.at[m], entry.at[m, zz, p], sem_entry_r.at[m, zz, p]
                    ).wait()
                acts[m, slot] = jnp.concatenate(
                    [entry[m, zz, p].astype(jnp.float32) for p in range(sections)], axis=0
                ).astype(jnp.bfloat16)

            @pl.when(s != 0)
            def _():
                wait_block(m, slot)

            for twin in range(1, cores):
                twin_copy(m, zz, twin).start()
        sums = half_dots(m, c)
        for twin in range(1, cores):
            other = lax.rem(c + twin, cores)
            for step in range(ring):
                wait_block(m, other * ring + lax.rem(z + step, ring))
            sums = [old + new for old, new in zip(sums, half_dots(m, other))]
        return sums

    def half_dots(m, core):
        span = ring * block
        columns = pl.ds(pl.multiple_of(core * span, 128), span)
        x = jnp.concatenate(
            [acts[m, core * ring + zz].astype(jnp.float32) for zz in range(ring)], axis=1
        )
        scaled = (x * gain_ref[:, columns]).astype(jnp.bfloat16)
        return [
            jnp.sum(x * x, axis=1, keepdims=True),
            *[matmul(step_w[d, :, columns], scaled, NT_DIMS) for d in range(2)],
            matmul(scaled, value_w[:, columns], NT_DIMS),
            matmul(scaled, mixed_w[0, columns, :]),
            matmul(scaled, mixed_w[1, columns, :]),
            matmul(scaled, gate_w[:, columns], NT_DIMS),
        ]

    def pre_copy(m, twin, zz):
        other = lax.rem(c + twin, cores)
        return remote(
            partial.at[m, twin - 1, zz],
            from_twin.at[m, twin - 1, zz],
            sem_pre_s.at[m, twin - 1, zz],
            sem_pre_r.at[m, twin - 1, zz],
            {"pp": s, "fs": z, "tp": other},
        )

    def rs_copy(m, step):
        zz = lax.rem(z + step, ring)
        return remote(
            pair_sum.at[m, zz],
            arrived.at[m, z],
            sem_rs_s.at[m, step - 1],
            sem_rs_r.at[m, z],
            {"pp": s, "fs": zz, "tp": c},
        )

    def mix(m, sums):
        squared, step_f, step_b, value_raw, write_raw, read_raw, gate_raw = sums
        scale = lax.rsqrt(squared / width + epsilon)
        scale_row = jnp.sum(jnp.where(diag, scale, 0.0), axis=0, keepdims=True)
        step_row = jnp.concatenate([step_f, step_b], axis=0) * scale_row + bias_col
        value_raw, write_raw = value_raw * scale, write_raw * scale
        read_raw, gate_raw = read_raw * scale, gate_raw * scale
        dt = jnp.maximum(step_row, 0.0) + jnp.log1p(jnp.exp(-jnp.abs(step_row)))
        a = dt * decay_col
        high = lax.Precision.HIGHEST
        fwd_row = matmul(a, tri_low, NT_DIMS, high)
        bwd_row = matmul(a, tri_up, NT_DIMS, high)
        fwd_col = matmul(tri_low, a, NT_DIMS, high)
        bwd_col = matmul(tri_up, a, NT_DIMS, high)
        pieces = inner // 128
        value = jnp.concatenate(
            [
                conv_act(
                    i,
                    value_raw[:, i * 128 : (i + 1) * 128],
                    [value_taps[k][:, i * 128 : (i + 1) * 128] for k in range(taps)],
                )
                for i in range(pieces)
            ],
            axis=1,
        )
        y = jnp.zeros((length, inner), jnp.float32)
        for g in range(groups):
            write = conv_act(
                pieces + 2 * g,
                write_raw[:, g * state : (g + 1) * state],
                [tap_w[k, g : g + 1, :] for k in range(taps)],
            )
            read = conv_act(
                pieces + 2 * g + 1,
                read_raw[:, g * state : (g + 1) * state],
                [tap_r[k, g : g + 1, :] for k in range(taps)],
            )
            scores = matmul(read, write, NT_DIMS)
            for e in range(per_group):
                h = g * per_group + e
                b = heads + h
                fwd_gap = fwd_col[:, h : h + 1] - fwd_row[h : h + 1, :]
                bwd_gap = bwd_col[:, b : b + 1] - bwd_row[b : b + 1, :]
                dt_f, dt_b = dt[h : h + 1, :], dt[b : b + 1, :]
                weight = jnp.exp(jnp.where(lower, fwd_gap, bwd_gap)) * jnp.where(
                    lower, dt_f, dt_b
                ) + jnp.where(diag, dt_b, 0.0)
                mixed = matmul((scores * weight).astype(jnp.bfloat16), value)
                y = jnp.where(lane_v // head == h, mixed, y)
        y = y + skip_row * value.astype(jnp.float32)
        gate = gate_raw.astype(jnp.bfloat16).astype(jnp.float32)
        gated = (y * silu(gate)).astype(jnp.bfloat16)
        span = ring * block

        def half_sums(core):
            start = pl.multiple_of(core * span, 128)
            return matmul(gated, out_w[:, pl.ds(start, span)])

        for twin in range(1, cores):
            sums = half_sums(lax.rem(c + twin, cores))
            for zz in range(ring):
                partial[m, twin - 1, zz] = sums[:, zz * block : (zz + 1) * block].astype(
                    jnp.bfloat16
                )
                pre_copy(m, twin, zz).start()
        sums = half_sums(c)
        for zz in range(ring):
            own_sum[m, zz] = sums[:, zz * block : (zz + 1) * block]

    def pair(m, zz):
        total = own_sum[m, zz]
        for twin in range(1, cores):
            pre_copy(m, twin, zz).wait_recv()
            total = total + from_twin[m, twin - 1, zz].astype(jnp.float32)
        return total

    def send_pairs(m):
        for step in far_first:
            zz = lax.rem(z + step, ring)
            pair_sum[m, zz] = pair(m, zz).astype(jnp.bfloat16)
            rs_copy(m, step).start()
        own_sum[m, z] = pair(m, z)

    def hop_copy(m, step):
        return remote(
            produced.at[m],
            acts.at[m, j],
            sem_hop_s.at[m, step],
            sem_ag_r.at[m, j],
            {"pp": lax.rem(s + 1, sections), "fs": lax.rem(z + step, ring), "tp": c},
        )

    def fin_copy(m, p):
        return remote(
            leaving.at[m, p],
            final_in.at[m],
            sem_fin_s.at[m, p],
            sem_fin_r.at[m],
            {"pp": p, "fs": z, "tp": c},
        )

    def sq_copy(m, step):
        other = lax.rem(me + step, sections * owners)
        return remote(
            squares.at[m],
            square_in.at[m, j],
            sem_sq_s.at[m, step - 1],
            sem_sq_r.at[m, j],
            place(other // owners, lax.rem(other, owners)),
        )

    def reduce(m):
        total = own_sum[m, z]
        for step in range(1, ring):
            source = lax.rem(z + step, ring)
            remote(
                pair_sum.at[m, source],
                arrived.at[m, source],
                sem_rs_s.at[m, step - 1],
                sem_rs_r.at[m, source],
                {"pp": s, "fs": source, "tp": c},
            ).wait_recv()
            total = total + arrived[m, source].astype(jnp.float32)
        branch = total.astype(jnp.bfloat16).astype(jnp.float32)
        made = (acts[m, j].astype(jnp.float32) + 0.5 * branch).astype(jnp.bfloat16)

        @pl.when(s != last)
        def _():
            produced[m] = made
            for step in (*far_first, 0):
                hop_copy(m, step).start()

        @pl.when(s == last)
        def _():
            o = made.astype(jnp.float32)
            for p in range(sections):
                leaving[m, p] = o[p * share : (p + 1) * share].astype(jnp.bfloat16)
            col = jnp.sum(o * o, axis=1, keepdims=True)
            full = jnp.concatenate(
                [
                    jnp.broadcast_to(col, (length, 128)),
                    jnp.zeros((128 - length, 128), jnp.float32),
                ],
                axis=0,
            )
            row = jnp.transpose(full)[0:1, :]
            squares[m] = row
            square_in[m, j] = row
            for p in range(last):
                fin_copy(m, p).start()
            for step in range(1, sections * owners):
                sq_copy(m, step).start()
            pltpu.make_async_copy(leaving.at[m, last], final_in.at[m], sem_local.at[m]).start()

    def finish(m):
        @pl.when(s != last)
        def _():
            fin_copy(m, 0).wait_recv()

        @pl.when(s == last)
        def _():
            pltpu.make_async_copy(leaving.at[m, last], final_in.at[m], sem_local.at[m]).wait()

        for k in range(owners):

            @pl.when((s != last) | (j != k))
            def _():
                remote(
                    squares.at[m],
                    square_in.at[m, k],
                    sem_sq_s.at[m, 0],
                    sem_sq_r.at[m, k],
                    place(last, k),
                ).wait_recv()

        total = square_in[m, 0]
        for k in range(1, owners):
            total = total + square_in[m, k]
        scale = lax.rsqrt(total / width + epsilon)
        column[m] = jnp.transpose(jnp.broadcast_to(scale, (128, 128)))
        own = column[m, pl.ds(pl.multiple_of(s * share, 8), share), :]
        out_ref[m] = (final_in[m].astype(jnp.float32) * own).astype(jnp.bfloat16)

    mix(0, receive(0))
    send_pairs(0)
    for m in range(1, micro):
        mix(m, receive(m))
        reduce(m - 1)
        send_pairs(m)
    reduce(micro - 1)
    for m in range(micro):
        finish(m)

    for m in range(micro):
        for step in range(1, ring):
            entry_copy(m, step).wait_send()
            rs_copy(m, step).wait_send()
        for twin in range(1, cores):
            for zz in range(ring):
                pre_copy(m, twin, zz).wait_send()
                twin_copy(m, zz, twin).wait_send()

        @pl.when(s != 0)
        def _():
            entry_copy(m, 0).wait_send()

        @pl.when(s != last)
        def _():
            for zz in range(ring):
                hop_copy(m, zz).wait_send()

        @pl.when(s == last)
        def _():
            for p in range(last):
                fin_copy(m, p).wait_send()
            for step in range(1, sections * owners):
                sq_copy(m, step).wait_send()


def fused_body(
    micro_in,
    norm_gain,
    proj_gate,
    proj_value,
    proj_write,
    proj_read,
    proj_step,
    step_bias,
    decay_log,
    skip_gain,
    conv_value,
    conv_write,
    conv_read,
    proj_out,
    sizes,
):
    sections, ring, cores = sizes["pp"], sizes["fs"], sizes["tp"]
    owners = ring * cores
    micro, share, block = micro_in.shape
    length = share * sections
    width = norm_gain.shape[1]
    taps = conv_value.shape[1]
    head = conv_value.shape[4]
    heads = conv_value.shape[2] * conv_value.shape[3]
    groups, state = conv_write.shape[2:]
    inner = heads * head
    args = (
        micro_in,
        norm_gain,
        jnp.transpose(proj_gate[0], (1, 2, 3, 0)).reshape(inner, width),
        jnp.transpose(proj_value[0], (1, 2, 3, 0)).reshape(inner, width),
        proj_write[0].reshape(width * groups, state),
        proj_read[0].reshape(width * groups, state),
        jnp.transpose(proj_step[0], (1, 2, 3, 0)).reshape(2, heads, width),
        step_bias[0].reshape(2, heads),
        decay_log[0].reshape(2, heads),
        skip_gain[0].reshape(heads),
        conv_value[0].reshape(taps, heads, head),
        conv_write[0],
        conv_read[0],
        proj_out[0].reshape(inner, width),
    )
    vmem = pl.BlockSpec(memory_space=pltpu.VMEM)
    smem = pl.BlockSpec(memory_space=pltpu.SMEM)
    whole = pl.BlockSpec(memory_space=pl.ANY)
    bf16, f32 = jnp.bfloat16, jnp.float32
    dma = pltpu.SemaphoreType.DMA
    pads = inner // 128 + 2 * groups
    return pl.pallas_call(
        functools.partial(relay_kernel, sizes),
        out_shape=jax.ShapeDtypeStruct(micro_in.shape, bf16),
        in_specs=[vmem] * 2 + [whole] * 4 + [vmem] + [smem] * 3 + [vmem] * 3 + [whole],
        out_specs=vmem,
        scratch_shapes=[
            pltpu.VMEM((inner, width), bf16),
            pltpu.VMEM((inner, width), bf16),
            pltpu.VMEM((2, width * groups, state), bf16),
            pltpu.VMEM((2, width, groups * state), bf16),
            pltpu.VMEM((inner, width), bf16),
            pltpu.VMEM((micro, ring, sections, share, block), bf16),
            pltpu.VMEM((micro, owners, length, block), bf16),
            pltpu.VMEM((micro, cores - 1, ring, length, block), bf16),
            pltpu.VMEM((micro, cores - 1, ring, length, block), bf16),
            pltpu.VMEM((micro, ring, length, block), f32),
            pltpu.VMEM((micro, ring, length, block), bf16),
            pltpu.VMEM((micro, ring, length, block), bf16),
            pltpu.VMEM((micro, length, block), bf16),
            pltpu.VMEM((micro, sections, share, block), bf16),
            pltpu.VMEM((micro, share, block), bf16),
            pltpu.VMEM((micro, 1, 128), f32),
            pltpu.VMEM((micro, owners, 1, 128), f32),
            pltpu.VMEM((micro, 128, 128), f32),
            pltpu.VMEM((pads, length + 16, 128), f32),
            dma((5,)),
            dma((micro, ring)),
            dma((micro, ring, sections)),
            dma((micro, cores - 1, ring)),
            dma((micro, cores - 1, ring)),
            dma((micro, ring - 1)),
            dma((micro, ring)),
            dma((micro, ring)),
            dma((micro, owners)),
            dma((micro, ring, cores - 1)),
            dma((micro, sections)),
            dma((micro,)),
            dma((micro, sections * owners - 1)),
            dma((micro, owners)),
            dma((micro,)),
        ],
        compiler_params=pltpu.CompilerParams(collective_id=0, has_side_effects=True),
    )(*args)


def solution(mesh):
    sizes = dict(mesh.shape)

    def chosen(micro_in, *weights):
        fits = micro_in.shape[2] % 128 == 0 and micro_in.shape[1] % 8 == 0 and 256 % weights[3].shape[2] == 0 and weights[3].shape[3] == 128
        return (fused_body if fits else body)(micro_in, *weights, *(() if not fits else (sizes,)))

    return jax.shard_map(
        chosen,
        mesh=mesh,
        in_specs=(
            P(None, "pp", ("tp", "fs")),
            P("pp", None),
            P("pp", None, "tp", "fs", None),
            P("pp", None, "tp", "fs", None),
            P("pp", None, "tp", None),
            P("pp", None, "tp", None),
            P("pp", None, None, "tp", "fs"),
            P("pp", None, "tp", "fs"),
            P("pp", None, "tp", "fs"),
            P("pp", "tp", "fs"),
            P("pp", None, "tp", "fs", None),
            P("pp", None, "tp", None),
            P("pp", None, "tp", None),
            P("pp", "tp", "fs", None, None),
        ),
        out_specs=P(None, "pp", ("tp", "fs")),
        check_vma=False,
    )
```
